32 devices in a mesh: sp: 8 (over z, x), tp: 4 (over y, core).
Axes of the slice: x: 2, y: 2, z: 4, core: 2. Of those that a mesh axis runs over, the one named last changes fastest.
Arguments:
- tokens: bfloat16 [8192, 2048], P('sp'), may hold values from -6 to 6
- pre_gain: float32 [2048], replicated, may hold values from 0.1 to 1.9
- w_query: bfloat16 [2048, 2048], P(None, 'tp'), may hold values from -0.125 to 0.125
- w_key: bfloat16 [2048, 2048], P(None, 'tp'), may hold values from -0.125 to 0.125
- w_value: bfloat16 [2048, 2048], P(None, 'tp'), may hold values from -0.125 to 0.125
- memory_output_gate_weight: bfloat16 [2048, 2048], P(None, 'tp'), may hold values from -0.125 to 0.125
- w_input_gate: bfloat16 [2048, 8], replicated, may hold values from -0.125 to 0.125
- w_forget_gate: bfloat16 [2048, 8], replicated, may hold values from -0.125 to 0.125
- input_bias: float32 [8], replicated, may hold values from -3 to 220
- forget_bias: float32 [8], replicated, may hold values from 3.9 to 12.4
- forget_extra: float32 [8192, 8], P('sp', 'tp'), may hold values from -1.5 to 0
- initial_memory: float32 [8, 256, 256], P('tp', 'sp'), may hold values from -2048 to 2048
- initial_normal: float32 [8, 256], P('tp', 'sp'), may hold values from -2048 to 2048
- memory_gain: float32 [2048], replicated, may hold values from 0.1 to 1.9
- w_pool_input: bfloat16 [2048, 1024], P(None, 'tp'), may hold values from -0.125 to 0.125
- w_pool_gate: bfloat16 [2048, 1024], P(None, 'tp'), may hold values from -0.125 to 0.125
- pool_mix: bfloat16 [8, 128, 128], replicated, may hold values from -0.5 to 0.5
- pool_gain: float32 [1024], replicated, may hold values from 0.1 to 1.9
- w_out_memory: bfloat16 [2048, 2048], P('tp'), may hold values from -0.109375 to 0.109375
- w_out_pool: bfloat16 [1024, 2048], P('tp'), may hold values from -0.109375 to 0.109375
- post_gain: float32 [2048], replicated, may hold values from 0.1 to 1.9
Outputs:
- layer_out: bfloat16 [8192, 2048], P(('sp', 'tp'))
The draws below stay inside these ranges and needn't reach their ends.
All inputs are finite; a program needn't handle non-finite values.
Results may differ from the reference program's by a relative error of at most 0.018.
The reference program's roundings to bfloat16 on the way count: a program that leaves them out, or rounds other values in their place, can miss the bound.
Values may be sent and summed in bfloat16 or wider, within the bound.
A program may use at most 128 MiB of HBM per device.

```python
import jax
import jax.numpy as jnp
from jax import lax

D = 2048
HEADS = 8
HEAD_DIM = 256
MEM_WIDTH = 2048
POOL_GROUPS = 8
GROUP_DIM = 128
POOL_WIDTH = 1024
TOKENS_PER_SHARD = 1024
BLOCK = 512
TOKENS = 8192
N_TP = 4


def draw_input_bias(key, part):
    result = jnp.clip(jax.random.normal(jax.random.fold_in(key, 13), (HEADS,), jnp.float32), -3.0, 3.0)
    return result


def draw_forget_bias(key, part):
    order = jax.random.permutation(jax.random.fold_in(key, 21), HEADS)
    fast_count = HEADS // 2
    slow_value = jnp.log(jnp.float32(TOKENS)) + 1.5 + jax.random.uniform(jax.random.fold_in(key, 22), (HEADS,), jnp.float32, -0.5, 0.5)
    slow_value = jnp.minimum(slow_value, 12.4)
    fast_value = jax.random.uniform(jax.random.fold_in(key, 23), (HEADS,), jnp.float32, 3.9, 4.6)
    return jnp.where(order < fast_count, fast_value, slow_value)


def draw_forget_extra(key, part):
    block_total = TOKENS // TOKENS_PER_SHARD
    rates = jnp.exp(jax.random.uniform(jax.random.fold_in(key, 31), (block_total, HEADS), jnp.float32, jnp.log(0.3), jnp.log(1.2)))
    rough = jax.random.uniform(jax.random.fold_in(key, 32), (TOKENS, HEADS), jnp.float32, 0.5, 1.5)
    baseline = -(jnp.repeat(rates, TOKENS_PER_SHARD, axis=0) * rough) / TOKENS
    spots = jax.random.randint(jax.random.fold_in(key, 33), (2,), 0, TOKENS)
    losses = jax.random.uniform(jax.random.fold_in(key, 34), (2, HEADS), jnp.float32, 0.22, 0.69)
    struck = (jnp.arange(TOKENS)[:, None] == spots[None, :]).astype(jnp.float32)
    return baseline - jnp.dot(struck, losses)


def block_scale(key, shape, pieces, least, top_value):
    def one(dim, parts):
        heights = jax.random.uniform(jax.random.fold_in(jax.random.fold_in(key, 6), dim), (parts,), jnp.float32, least / len(pieces), top_value / len(pieces))
        return jnp.repeat(jnp.exp(heights), shape[dim] // parts).reshape((-1,) + (1,) * (len(shape) - dim - 1))

    factor_of = one(*pieces[0])
    for cut in pieces[1:]:
        factor_of = factor_of * one(*cut)
    return factor_of


def scatter_about(own_key, shape, deviation, limit, shards=(), dtype=jnp.bfloat16):
    values = deviation * jax.random.normal(own_key, shape, jnp.float32)
    if shards:
        values = values * block_scale(own_key, shape, shards, -0.22, 0.18)
    return jnp.clip(values, -limit, limit).astype(dtype)


def setup_inputs(seed: int = 0) -> dict:
    streams_of = jax.random.split(jax.random.key(seed), 22)
    tokens = scatter_about(streams_of[0], (TOKENS, D), 1.0, 6.0, ((0, 8),))
    pre_gain = jnp.clip(1.0 + 0.18 * jax.random.normal(streams_of[1], (D,), jnp.float32), 0.1, 1.9)
    w_query = scatter_about(streams_of[2], (D, MEM_WIDTH), D ** -0.5, 0.125, ((1, 4),))
    w_key = scatter_about(streams_of[3], (D, MEM_WIDTH), D ** -0.5, 0.125, ((1, 4),))
    w_value = scatter_about(streams_of[4], (D, MEM_WIDTH), D ** -0.5, 0.125, ((1, 4),))
    memory_output_gate_weight = scatter_about(streams_of[5], (D, MEM_WIDTH), D ** -0.5, 0.125, ((1, 4),))
    w_input_gate = scatter_about(streams_of[6], (D, HEADS), D ** -0.5, 0.125)
    w_forget_gate = scatter_about(streams_of[7], (D, HEADS), D ** -0.5, 0.125)
    input_bias = draw_input_bias(jax.random.fold_in(streams_of[21], 71), 0)
    forget_bias = draw_forget_bias(jax.random.fold_in(streams_of[21], 71), 0)
    forget_extra = draw_forget_extra(jax.random.fold_in(streams_of[21], 71), 0)
    initial_memory = scatter_about(streams_of[11], (HEADS, HEAD_DIM, HEAD_DIM), (4 * TOKENS ** 0.5), 2048.0, ((0, 4), (1, 8)), jnp.float32)
    initial_normal = scatter_about(streams_of[12], (HEADS, HEAD_DIM), (4 * TOKENS ** 0.5), 2048.0, ((0, 4), (1, 8)), jnp.float32)
    memory_gain = jnp.clip(1.0 + 0.18 * jax.random.normal(streams_of[13], (MEM_WIDTH,), jnp.float32), 0.1, 1.9)
    w_pool_input = scatter_about(streams_of[14], (D, POOL_WIDTH), D ** -0.5, 0.125, ((1, 4),))
    w_pool_gate = scatter_about(streams_of[15], (D, POOL_WIDTH), D ** -0.5, 0.125, ((1, 4),))
    pool_mix = scatter_about(streams_of[16], (POOL_GROUPS, GROUP_DIM, GROUP_DIM), GROUP_DIM ** -0.5, 0.5)
    pool_gain = jnp.clip(1.0 + 0.18 * jax.random.normal(streams_of[17], (POOL_WIDTH,), jnp.float32), 0.1, 1.9)
    w_out_memory = scatter_about(streams_of[18], (MEM_WIDTH, D), (MEM_WIDTH + POOL_WIDTH) ** -0.5, 0.109375, ((0, 4),))
    w_out_pool = scatter_about(streams_of[19], (POOL_WIDTH, D), (MEM_WIDTH + POOL_WIDTH) ** -0.5, 0.109375, ((0, 4),))
    post_gain = jnp.clip(1.0 + 0.18 * jax.random.normal(streams_of[20], (D,), jnp.float32), 0.1, 1.9)
    return dict(tokens=tokens, pre_gain=pre_gain, w_query=w_query, w_key=w_key, w_value=w_value, memory_output_gate_weight=memory_output_gate_weight, w_input_gate=w_input_gate, w_forget_gate=w_forget_gate, input_bias=input_bias, forget_bias=forget_bias, forget_extra=forget_extra, initial_memory=initial_memory, initial_normal=initial_normal, memory_gain=memory_gain, w_pool_input=w_pool_input, w_pool_gate=w_pool_gate, pool_mix=pool_mix, pool_gain=pool_gain, w_out_memory=w_out_memory, w_out_pool=w_out_pool, post_gain=post_gain)


EPS = 1e-06

def normalize(values, gain):
    return values * lax.rsqrt(lax.optimization_barrier(jnp.mean(values * values, axis=-1, keepdims=True)) + EPS) * gain

def block_parts(memory_carry, block_inputs):
    matrix_memory_state, memory_normal, stabilizer = memory_carry
    queries, keys_in, incoming_values, log_input, log_keep = block_inputs
    length = queries.shape[1]
    head_scale = queries.shape[2] ** (-0.5)
    causal = jnp.arange(length)[:, None] >= jnp.arange(length)[None, :]
    running_keep = jnp.cumsum(log_keep, axis=-1)
    decayed = jnp.where(causal[None], running_keep[:, :, None] - running_keep[:, None, :] + log_input[:, None, :], -jnp.inf)
    carried = running_keep + stabilizer[:, None]
    row_max = jnp.maximum(lax.optimization_barrier(jnp.max(decayed, axis=-1)), carried)
    wide_queries = queries.astype(jnp.float32)
    broadcast_values = incoming_values.astype(jnp.float32)
    wide_keys = keys_in.astype(jnp.float32)
    scores = jnp.einsum('hld,hsd->hls', wide_queries, wide_keys)
    weights = jnp.exp(decayed - row_max[:, :, None]) * scores * head_scale
    carry_weight = jnp.exp(carried - row_max) * head_scale
    rounded = lax.optimization_barrier(weights.astype(jnp.bfloat16)).astype(jnp.float32)
    numerator = jnp.einsum('hls,hsd->hld', rounded, broadcast_values)
    numerator = numerator + carry_weight[:, :, None] * jnp.einsum('hld,hde->hle', wide_queries, matrix_memory_state, precision=lax.Precision.HIGHEST)
    denominator = lax.optimization_barrier(jnp.sum(weights, axis=-1)) + carry_weight * jnp.einsum('hld,hd->hl', wide_queries, memory_normal, precision=lax.Precision.HIGHEST)
    block_keep = running_keep[:, -1]
    write_log = block_keep[:, None] - running_keep + log_input
    new_stabilizer = jnp.maximum(block_keep + stabilizer, lax.optimization_barrier(jnp.max(write_log, axis=-1)))
    decay_factor = jnp.exp(block_keep + stabilizer - new_stabilizer)
    write_weight = jnp.exp(write_log - new_stabilizer[:, None])
    key_projected = write_weight[:, :, None] * wide_keys
    key_projected_rounded = lax.optimization_barrier(key_projected.astype(jnp.bfloat16)).astype(jnp.float32)
    matrix_memory_state = decay_factor[:, None, None] * matrix_memory_state + jnp.einsum('gbq,gbd->gqd', key_projected_rounded, broadcast_values)
    memory_normal = decay_factor[:, None] * memory_normal + lax.optimization_barrier(jnp.sum(key_projected, axis=1))
    return ((matrix_memory_state, memory_normal, new_stabilizer), (numerator, denominator, row_max))

def reference(tokens, pre_gain, w_query, w_key, w_value, memory_output_gate_weight, w_input_gate, w_forget_gate, input_bias, forget_bias, forget_extra, initial_memory, initial_normal, memory_gain, w_pool_input, w_pool_gate, pool_mix, pool_gain, w_out_memory, w_out_pool, post_gain):
    normed = normalize(tokens.astype(jnp.float32), pre_gain).astype(jnp.bfloat16)

    def by_heads(weight):
        product = jnp.dot(normed, weight, preferred_element_type=jnp.float32)
        return product.reshape(TOKENS, HEADS, HEAD_DIM).transpose(1, 0, 2)
    queries = by_heads(w_query).astype(jnp.bfloat16)
    keys_all = by_heads(w_key).astype(jnp.bfloat16)
    values_all = by_heads(w_value).astype(jnp.bfloat16)
    memory_gate = by_heads(memory_output_gate_weight)
    log_input = (jnp.dot(normed, w_input_gate, preferred_element_type=jnp.float32) + input_bias).T
    log_keep = (jax.nn.log_sigmoid(jnp.dot(normed, w_forget_gate, preferred_element_type=jnp.float32) + forget_bias) + forget_extra).T
    block_total = TOKENS // BLOCK

    def split(array):
        return jnp.moveaxis(array.reshape((HEADS, block_total, BLOCK) + array.shape[2:]), 1, 0)

    def join(array):
        return jnp.moveaxis(array, 0, 1).reshape((HEADS, TOKENS) + array.shape[3:])
    begin = (initial_memory, initial_normal, jnp.zeros((HEADS,), jnp.float32))
    _, (numerator, denominator, row_max) = lax.scan(block_parts, begin, (split(queries), split(keys_all), split(values_all), split(log_input), split(log_keep)))
    numerator, denominator, row_max = (join(numerator), join(denominator), join(row_max))
    memory_rows = numerator / jnp.maximum(jnp.abs(denominator), jnp.exp(-row_max))[..., None]
    row_scale = lax.rsqrt(lax.optimization_barrier(jnp.mean(memory_rows * memory_rows, axis=(0, 2), keepdims=True)) + EPS)
    memory_out = (memory_rows * row_scale * memory_gain.reshape(HEADS, 1, HEAD_DIM) * jax.nn.silu(memory_gate)).astype(jnp.bfloat16)
    memory_out = memory_out.transpose(1, 0, 2).reshape(TOKENS, MEM_WIDTH)
    pool_input = jnp.dot(normed, w_pool_input, preferred_element_type=jnp.float32).astype(jnp.bfloat16)
    grouped = pool_input.astype(jnp.float32).reshape(TOKENS, POOL_GROUPS, GROUP_DIM)
    running = jnp.concatenate([jnp.zeros((1, POOL_GROUPS, GROUP_DIM), jnp.float32), jnp.cumsum(grouped, axis=0)], axis=0)
    position = (jnp.arange(TOKENS) + 1).astype(jnp.int32)[:, None]
    windows = (2 ** (jnp.arange(POOL_GROUPS) + 1)).astype(jnp.int32)[None, :]
    lowest = jnp.maximum(position - windows, 0).astype(jnp.int32)
    group_ids = jnp.arange(POOL_GROUPS).astype(jnp.int32)[None, :]
    window_sums = running[1:] - running[lowest, group_ids]
    counts = (position - lowest).astype(jnp.float32)
    pooled = (window_sums / counts[..., None] - grouped).astype(jnp.bfloat16)
    mixed = jnp.einsum('tgc,gce->tge', pooled.astype(jnp.float32), pool_mix.astype(jnp.float32))
    pool_gate = jnp.dot(normed, w_pool_gate, preferred_element_type=jnp.float32)
    pool_out = (mixed.reshape(TOKENS, POOL_WIDTH) * pool_gain * jax.nn.silu(pool_gate)).astype(jnp.bfloat16)
    memory_cols = MEM_WIDTH // N_TP
    pool_cols = POOL_WIDTH // N_TP
    summed = jnp.zeros((TOKENS, D), jnp.float32)
    for member in range(N_TP):
        low_mem = member * memory_cols
        low_pool = member * pool_cols
        partial_value = jnp.dot(memory_out[:, low_mem:low_mem + memory_cols], w_out_memory[low_mem:low_mem + memory_cols], preferred_element_type=jnp.float32)
        partial_value = partial_value + jnp.dot(pool_out[:, low_pool:low_pool + pool_cols], w_out_pool[low_pool:low_pool + pool_cols], preferred_element_type=jnp.float32)
        summed = summed + lax.optimization_barrier(partial_value.astype(jnp.bfloat16)).astype(jnp.float32)
    return normalize(summed, post_gain).astype(jnp.bfloat16)
```

```python
import functools
import types

import jax
import jax.numpy as jnp
from jax import lax
from jax.experimental import pallas as pl
from jax.experimental.pallas import tpu as pltpu
from jax.sharding import PartitionSpec as P

HEAD_DIM = 256
GROUP_DIM = 128
WIDEST = 256
TILE = 256
CHUNKS = 4
QUAD = 4
SUB = 64
EPS = 1e-06
FLOOR = -1e30
F32 = jnp.float32
BF16 = jnp.bfloat16
MESH = pl.DeviceIdType.MESH
INPUTS = 21


def dot(a, b):
    return jnp.dot(a, b, preferred_element_type=F32)


def dot_t(a, b):
    return lax.dot_general(a, b, (((1,), (1,)), ((), ())), preferred_element_type=F32)


def silu(x):
    return x / (1.0 + jnp.exp(-x))


def kernel(n_sp, n_tp, names, *refs):
    (
        tokens_hbm,
        gain_hbm,
        wq_hbm,
        wk_hbm,
        wv_hbm,
        wg_hbm,
        w_in_hbm,
        w_forget_hbm,
        b_in_hbm,
        b_forget_hbm,
        extra_hbm,
        init_hbm,
        normal_hbm,
        mem_gain_hbm,
        wpi_hbm,
        wpg_hbm,
        mix_hbm,
        pool_gain_hbm,
        wom_hbm,
        wop_hbm,
        post_hbm,
    ) = refs[:INPUTS]
    out_hbm = refs[INPUTS]
    r = types.SimpleNamespace(**dict(zip(names, refs[INPUTS + 1 :])))
    T, D = r.tokens.shape
    H = r.q.shape[0]
    G = r.mix.shape[0]
    heads = r.w_in.shape[0]
    sp = lax.axis_index("sp")
    tp = lax.axis_index("tp")
    head_scale = HEAD_DIM ** (-0.5)
    tiles = T // TILE
    quad = r.e_recv.shape[1]
    rows_own = HEAD_DIM // quad
    quads = n_sp // quad
    my_quad, my_slot = sp // quad, lax.rem(sp, quad)
    part = HEAD_DIM // n_sp

    mem_lanes = pl.ds(pl.multiple_of(tp * H * HEAD_DIM, HEAD_DIM), H * HEAD_DIM)
    pool_lanes = pl.ds(pl.multiple_of(tp * G * GROUP_DIM, GROUP_DIM), G * GROUP_DIM)
    loads = {}

    def load(name, src, dst):
        loads[name] = pltpu.make_async_copy(src, dst, r.local_sem.at[len(loads)])
        loads[name].start()

    load("gain", gain_hbm, r.gain)

    def load_tokens(t):
        span = pl.ds(t * TILE, TILE)
        load(("tokens", t), tokens_hbm.at[span], r.tokens.at[span])

    def load_head(name, source, target, h):
        lanes = pl.ds(h * HEAD_DIM, HEAD_DIM)
        load((name, h), source.at[:, lanes], target.at[:, lanes])

    for t in range(tiles // 2):
        load_tokens(t)
    load("w_in", w_in_hbm, r.w_in)
    load("w_forget", w_forget_hbm, r.w_forget)
    load("b_in", b_in_hbm, r.b_in)
    load("b_forget", b_forget_hbm, r.b_forget)
    load_head("wk", wk_hbm, r.wk, 0)
    for t in range(tiles // 2, tiles):
        load_tokens(t)
    load_head("wv", wv_hbm, r.wv, 0)
    load("extra", extra_hbm, r.extra)
    load("normal", normal_hbm, r.normal)
    for h in range(1, H):
        load_head("wk", wk_hbm, r.wk, h)
        load_head("wv", wv_hbm, r.wv, h)
    load("wpi", wpi_hbm, r.wpi)
    load("wq", wq_hbm, r.wq)
    load("wpg", wpg_hbm, r.wpg)
    load("wg", wg_hbm, r.wg)
    load("mix", mix_hbm.at[pl.ds(tp * G, G)], r.mix)
    load("pool_gain", pool_gain_hbm.at[:, pool_lanes], r.pool_gain)
    load("mem_gain", mem_gain_hbm.at[:, mem_lanes], r.mem_gain)
    load("wop", wop_hbm, r.wop)
    load("wom", wom_hbm, r.wom)
    load("post", post_hbm, r.post)

    barrier = pltpu.get_barrier_semaphore()
    for step in range(1, n_sp):
        pl.semaphore_signal(
            barrier, inc=1, device_id={"sp": lax.rem(sp + step, n_sp)}, device_id_type=MESH
        )
    for step in range(1, n_tp):
        pl.semaphore_signal(
            barrier, inc=1, device_id={"tp": lax.rem(tp + step, n_tp)}, device_id_type=MESH
        )

    def remote(src, dst, send_sem, recv_sem, axis, peer):
        return pltpu.make_async_remote_copy(
            src_ref=src,
            dst_ref=dst,
            send_sem=send_sem,
            recv_sem=recv_sem,
            device_id={axis: peer},
            device_id_type=MESH,
        )

    r.gates_w[...] = jnp.zeros_like(r.gates_w)
    r.gates_b[...] = jnp.zeros_like(r.gates_b)
    r.rows[...] = jnp.zeros_like(r.rows)
    r.a_send[...] = jnp.zeros_like(r.a_send)
    loads["gain"].wait()
    loads["tokens", 0].wait()

    def norm_tile(rows):
        x = r.tokens[rows, :].astype(F32)
        scale = lax.rsqrt(jnp.mean(x * x, axis=-1, keepdims=True) + EPS)
        r.normed[rows, :] = (x * scale * r.gain[...]).astype(BF16)

    def head_lanes(h):
        return slice(h * HEAD_DIM, (h + 1) * HEAD_DIM)

    def whole(ref, h):
        return lambda rows, value: ref.__setitem__((h, rows), value.astype(ref.dtype))

    def gates_product(rows):
        r.cols[rows, :] = dot_t(r.normed[rows, :], r.gates_w[...]) + r.gates_b[...]

    def product(weight, lanes, rows, store):
        store(rows, dot(r.normed[rows, :], weight[:, lanes]))

    per_owner = n_sp // quad
    owner = sp // per_owner
    turn = lax.rem(sp, per_owner)
    init_place = r.init.at[:, pl.ds(pl.multiple_of(turn * part, part), part), :]
    init_copy = remote(
        init_hbm, init_place, r.init_sems.at[per_owner], r.init_sems.at[turn], "sp", owner
    )
    init_local = pltpu.make_async_copy(init_hbm, init_place, r.init_sems.at[per_owner])

    def send_init():
        pl.semaphore_wait(barrier, n_sp - 1 + n_tp - 1)

        @pl.when(owner != sp)
        def _():
            init_copy.start()

        @pl.when(owner == sp)
        def _():
            init_local.start()

    half = tiles // 2
    for t in range(half):
        if t > 0:
            loads["tokens", t].wait()
        for sub in range(0, TILE, SUB):
            norm_tile(pl.ds(t * TILE + sub, SUB))
    for name in ("w_in", "w_forget", "b_in", "b_forget", ("wk", 0)):
        loads[name].wait()
    r.gates_w[0:heads, :] = r.w_in[...]
    r.gates_w[heads : 2 * heads, :] = r.w_forget[...]
    r.gates_b[:, 0:heads] = r.b_in[...]
    r.gates_b[:, heads : 2 * heads] = r.b_forget[...]
    for t in range(half, tiles):
        loads["tokens", t].wait()

    def early_products(rows):
        gates_product(rows)
        product(r.wk, head_lanes(0), rows, whole(r.k, 0))

    pieces = (slice(0, half * TILE), slice(half * TILE, T))
    early_products(pieces[0])
    for t in range(half, tiles):
        for sub in range(0, TILE, SUB):
            norm_tile(pl.ds(t * TILE + sub, SUB))
    for name in (("wv", 0), "extra", "normal"):
        loads[name].wait()
    early_products(pieces[1])
    send_init()
    for rows in pieces:
        product(r.wv, head_lanes(0), rows, whole(r.v, 0))

    tri = (
        lax.broadcasted_iota(jnp.int32, (TILE, TILE), 0)
        <= lax.broadcasted_iota(jnp.int32, (TILE, TILE), 1)
    ).astype(F32)
    carry = jnp.zeros((8, 1), F32)
    for t in range(tiles):
        span = pl.ds(t * TILE, TILE)
        r.raw[:, span] = r.cols[span, :].T
        own_rows = [r.raw[pl.ds(heads + tp * H + h, 1), span] for h in range(H)]
        added = [r.extra[h : h + 1, span] for h in range(H)]
        spare = [jnp.zeros((8 - H, TILE), F32)]
        raw = jnp.concatenate(own_rows + spare, axis=0)
        log_keep = jnp.minimum(raw, 0.0) - jnp.log1p(jnp.exp(-jnp.abs(raw)))
        log_keep = log_keep + jnp.concatenate(added + spare, axis=0)
        run = carry + jnp.dot(
            log_keep, tri, preferred_element_type=F32, precision=lax.Precision.HIGHEST
        )
        carry = run[:, TILE - 1 : TILE]
        for h in range(H):
            keep = run[h : h + 1]
            r.rows[h : h + 1, span] = r.raw[pl.ds(tp * H + h, 1), span] - keep
            r.rows[H + h : H + h + 1, span] = keep
    for t in range(tiles):
        span = pl.ds(t * TILE, TILE)
        r.cols[span, :] = r.rows[:, span].T

    def a_copy(h, step):
        peer = lax.rem(sp + step, n_sp)
        return remote(
            r.a_send.at[h], r.a_recv.at[sp, h], r.a_sems.at[0, h, step], r.a_sems.at[1, h, step], "sp", peer
        )

    def s_copy(h, step):
        peer = lax.rem(my_slot + step, quad)
        return remote(
            r.s_send.at[h, peer],
            r.s_recv.at[h, my_slot],
            r.s_sems.at[0, h, step],
            r.s_sems.at[1, h, step],
            "sp",
            my_quad * quad + peer,
        )

    def e_copy(h, step):
        peer = lax.rem(my_slot + step, quad)
        return remote(
            r.e_send.at[h, peer],
            r.e_recv.at[h, my_slot],
            r.e_sems.at[0, h, step],
            r.e_sems.at[1, h, step],
            "sp",
            my_quad * quad + peer,
        )

    def t_copy(h):
        return remote(
            r.t_send.at[h],
            r.t_recv.at[h],
            r.t_sems.at[0, h],
            r.t_sems.at[1, h],
            "sp",
            lax.rem(sp + quad, n_sp),
        )

    for h in range(H):
        if h > 0:
            loads["wk", h].wait()
            loads["wv", h].wait()
            product(r.wk, head_lanes(h), slice(0, T), whole(r.k, h))
            product(r.wv, head_lanes(h), slice(0, T), whole(r.v, h))
        a_max = jnp.max(r.rows[h : h + 1, :], axis=-1, keepdims=True)
        total = r.rows[H + h : H + h + 1, T - 1 : T]
        state = jnp.zeros((HEAD_DIM, HEAD_DIM), F32)
        normal = jnp.zeros((1, HEAD_DIM), F32)
        for t in range(tiles):
            span = pl.ds(t * TILE, TILE)
            weight = jnp.exp(r.cols[span, h : h + 1] - a_max)
            kw = weight * r.k[h, span, :].astype(F32)
            normal = normal + jnp.sum(kw, axis=0, keepdims=True)
            state = state + lax.dot_general(
                kw.astype(BF16),
                r.v[h, span, :],
                (((0,), (0,)), ((), ())),
                preferred_element_type=F32,
            )
        r.s_send[h] = state.reshape(quad, rows_own, HEAD_DIM).astype(BF16)
        r.a_send[h, 0:1, :] = jnp.broadcast_to(total + a_max, (1, HEAD_DIM))
        r.a_send[h, 1:2, :] = jnp.broadcast_to(total, (1, HEAD_DIM))
        r.a_send[h, 2:3, :] = normal
        r.a_send[h, 3:4, 0:part] = r.normal[h : h + 1, :]
        for step in range(1, n_sp):
            a_copy(h, step).start()
        for step in range(1, quad):
            s_copy(h, step).start()
        r.s_recv[h, my_slot] = r.s_send[h, my_slot]
        r.a_recv[sp, h] = r.a_send[h]

    def m_row(h, j):
        return pl.ds(h * (n_sp + 1) + j, 1)

    def chain(h):
        for step in range(1, n_sp):
            a_copy(h, step).wait()
        for j in range(n_sp):
            r.start[h : h + 1, j * part : (j + 1) * part] = r.a_recv[j, h, 3:4, 0:part]
        normal = r.start[h : h + 1, :]
        stab = jnp.zeros((1, HEAD_DIM), F32)
        my_stab, my_normal = stab, normal
        for j in range(n_sp):
            r.m[m_row(h, j), :] = stab
            if j > 0:
                my_stab = jnp.where(sp == j, stab, my_stab)
                my_normal = jnp.where(sp == j, normal, my_normal)
            late = r.a_recv[j, h, 0:1, :]
            keep = r.a_recv[j, h, 1:2, :]
            joint = jnp.maximum(late, keep + stab)
            normal = normal * jnp.exp(keep + stab - joint) + r.a_recv[j, h, 2:3, :] * jnp.exp(
                late - joint
            )
            stab = joint
        r.m[m_row(h, n_sp), :] = stab
        r.enter[h : h + 1, :] = my_stab
        r.enter[H + h : H + h + 1, :] = my_normal

    def spread(h):
        state = r.state[h]
        for i in range(quad):
            j = my_quad * quad + i
            r.e_send[h, i] = state.astype(BF16)
            stab, joint = r.m[m_row(h, j), :], r.m[m_row(h, j + 1), :]
            late = r.a_recv[j, h, 0:1, :]
            keep = r.a_recv[j, h, 1:2, :]
            state = state * jnp.exp(keep + stab - joint) + r.s_recv[h, i].astype(F32) * jnp.exp(
                late - joint
            )
        r.t_send[h] = state.astype(BF16)

        @pl.when(my_quad < quads - 1)
        def _():
            t_copy(h).start()

        for step in range(1, quad):
            e_copy(h, step).start()
        r.e_recv[h, my_slot] = r.e_send[h, my_slot]

    def gathered(h):
        chain(h)
        for step in range(1, quad):
            s_copy(h, step).wait()

        @pl.when(my_quad == 0)
        def _():
            if h == 0:
                for turn_in in range(per_owner):
                    source = sp * per_owner + turn_in

                    @pl.when(source != sp)
                    def _():
                        init_copy_from(turn_in).wait_recv()

                @pl.when(owner == sp)
                def _():
                    init_local.wait()

            r.state[h] = r.init[h]
            spread(h)

    def init_copy_from(turn_in):
        place = r.init.at[:, pl.ds(turn_in * part, part), :]
        return remote(init_hbm, place, r.init_sems.at[per_owner], r.init_sems.at[turn_in], "sp", owner)

    def carried_on(h):
        @pl.when(my_quad > 0)
        def _():
            t_copy(h).wait_recv()
            r.state[h] = r.t_recv[h].astype(F32)
            spread(h)

    loads["wq"].wait()

    def query_to(h):
        def store(rows, value):
            r.q[h, rows, :] = value.astype(BF16) * head_scale

        return store

    for h in range(H):
        product(r.wq, head_lanes(h), slice(0, T), query_to(h))
    gathered(0)
    loads["wpi"].wait()

    def store_pool(rows, value):
        r.ext[WIDEST + rows.start : WIDEST + rows.stop, :] = value.astype(BF16)

    for piece in range(2):
        product(r.wpi, slice(None), slice(piece * T // 2, (piece + 1) * T // 2), store_pool)
    halo = remote(
        r.ext.at[pl.ds(T, WIDEST)],
        r.ext.at[pl.ds(0, WIDEST)],
        r.halo_sems.at[0],
        r.halo_sems.at[1],
        "sp",
        lax.rem(sp + 1, n_sp),
    )
    for h in range(1, H):
        gathered(h)
    halo.start()

    for name in ("wg", "mem_gain", "wpg", "pool_gain", "mix"):
        loads[name].wait()
    chips = n_tp // 2
    chip, core = tp // 2, lax.rem(tp, 2)
    sibling = chip * 2 + 1 - core
    block = T // n_tp
    segment = 2 * block

    def gate_to(h):
        def store(rows, value):
            r.gate[h, rows, :] = r.mem_gain[:, head_lanes(h)] * silu(value)

        return store

    def store_gate(rows, value):
        r.pgate[rows, :] = r.pool_gain[...] * silu(value)

    def gates_of(target):
        start = pl.multiple_of(target * segment, segment)
        for h in range(H):
            product(r.wg, head_lanes(h), pl.ds(start, segment), gate_to(h))
        for piece in range(2):
            rows = pl.ds(pl.multiple_of(start + piece * block, block), block)
            product(r.wpg, slice(None), rows, store_gate)

    for j in range(1, chips):
        gates_of(lax.rem(chip + j, chips))
    carried_on(0)
    diag_mask = lax.broadcasted_iota(jnp.int32, (TILE, TILE), 0) >= lax.broadcasted_iota(
        jnp.int32, (TILE, TILE), 1
    )

    def attend(h):
        enter_max = r.enter[h : h + 1, 0:1]
        enter_normal = r.enter[H + h : H + h + 1, :]
        for t in range(tiles):
            span = pl.ds(t * TILE, TILE)
            queries = r.q[h, span, :]
            near = jnp.where(diag_mask, r.rows[h : h + 1, span], FLOOR)
            top = jnp.max(near, axis=-1, keepdims=True)
            if t > 0:
                far = r.rows[h : h + 1, 0 : t * TILE]
                top = jnp.maximum(top, jnp.max(far, axis=-1, keepdims=True))
            weights = jnp.exp(near - top) * dot_t(queries, r.k[h, span, :])
            den = jnp.sum(weights, axis=-1, keepdims=True)
            num = dot(weights.astype(BF16), r.v[h, span, :])
            if t > 0:
                weights = jnp.exp(far - top) * dot_t(queries, r.k[h, 0 : t * TILE, :])
                den = den + jnp.sum(weights, axis=-1, keepdims=True)
                num = num + dot(weights.astype(BF16), r.v[h, 0 : t * TILE, :])
            keep = r.cols[span, H + h : H + h + 1]
            row_max = keep + top
            carried = keep + enter_max
            joint = jnp.maximum(row_max, carried)
            local_weight = jnp.exp(row_max - joint)
            carry_weight = jnp.exp(carried - joint)
            den = den * local_weight + carry_weight * jnp.sum(
                queries.astype(F32) * enter_normal, axis=-1, keepdims=True
            )
            bound = jnp.maximum(jnp.abs(den), jnp.exp(-joint))
            r.num[h, span, :] = num * (local_weight / bound)
            r.beta[h, span, :] = carry_weight / bound

    attend(0)
    for h in range(1, H):
        carried_on(h)
    for h in range(1, H):
        attend(h)
    halo.wait()

    def pool_of(target):
        for g in range(G):
            window = jnp.left_shift(2, tp * G + g)
            offset = (
                lax.broadcasted_iota(jnp.int32, (TILE, TILE + WIDEST), 0)
                + WIDEST
                - lax.broadcasted_iota(jnp.int32, (TILE, TILE + WIDEST), 1)
            )
            band = jnp.where((offset >= 0) & (offset < window), 1.0, 0.0).astype(BF16)
            lanes = slice(g * GROUP_DIM, (g + 1) * GROUP_DIM)
            for piece in range(segment // TILE):
                start = pl.multiple_of(target * segment + piece * TILE, TILE)
                span = pl.ds(start, TILE)
                here = r.ext[pl.ds(pl.multiple_of(start + WIDEST, TILE), TILE), lanes]
                before = r.ext[pl.ds(start, WIDEST), lanes]
                before = jnp.where(sp + start > 0, before.astype(F32), 0.0).astype(BF16)
                sums = dot(band[:, :WIDEST], before) + dot(band[:, WIDEST:], here)
                position = lax.broadcasted_iota(jnp.int32, (TILE, 1), 0) + (sp * T + start + 1)
                counts = jnp.minimum(position, window).astype(F32)
                pooled = (sums / counts - here.astype(F32)).astype(BF16)
                r.pool[span, lanes] = (dot(pooled, r.mix[g]) * r.pgate[span, lanes]).astype(BF16)

    for j in range(1, chips):
        pool_of(lax.rem(chip + j, chips))
    loads["wop"].wait()
    loads["wom"].wait()
    loads["post"].wait()
    size = block // CHUNKS
    slots = chips * CHUNKS

    def chunk_rows(target, which, n):
        return pl.ds(pl.multiple_of((target * 2 + which) * block + n * size, size), size)

    def memory_product(rows):
        parts = [(r.num[h, rows, :] * r.gate[h, rows, :]).astype(BF16) for h in range(H)]
        return dot(parts[0] if H == 1 else jnp.concatenate(parts, axis=1), r.wom[...])

    def finish(rows):
        pool = dot(r.pool[rows, :], r.wop[...])
        return (memory_product(rows) * r.scale[rows, 0:1] + pool).astype(BF16)

    jobs = []
    for j in range(1, chips + 1):
        for n in range(CHUNKS):
            jobs.append((j, n, lax.rem(chip + j, chips), (j - 1) * CHUNKS + n))

    siblings, links = {}, {}

    def to_sibling(slot):
        siblings[slot] = remote(
            r.sib_send.at[slot],
            r.sib_recv.at[slot],
            r.sib_sems.at[0, slot],
            r.sib_sems.at[1, slot],
            "tp",
            sibling,
        )
        siblings[slot].start()

    def to_chip(slot, target):
        links[slot] = remote(
            r.link_send.at[slot],
            r.link_recv.at[slot],
            r.link_sems.at[0, slot],
            r.link_sems.at[1, slot],
            "tp",
            target * 2 + core,
        )
        links[slot].start()

    lead_theirs = chunk_rows(jobs[0][2], 1 - core, 0)
    lead_ours = chunk_rows(jobs[0][2], core, 0)
    r.sib_send[slots] = dot(r.pool[lead_theirs, :], r.wop[...]).astype(BF16)
    to_sibling(slots)
    r.lead_pool[...] = dot(r.pool[lead_ours, :], r.wop[...])

    def piece_spans(n):
        return [slice(b * block + n * size, b * block + (n + 1) * size) for b in range(n_tp)]

    def combine(h, n):
        spans = piece_spans(n)
        state = r.e_recv[h].reshape(HEAD_DIM, HEAD_DIM)
        carried = dot(jnp.concatenate([r.q[h, span, :] for span in spans], axis=0), state)
        squares = []
        for b, span in enumerate(spans):
            memory = r.num[h, span, :] + r.beta[h, span, :] * carried[b * size : (b + 1) * size]
            r.num[h, span, :] = memory
            squares.append(jnp.sum(memory * memory, axis=-1, keepdims=True))
        squares = jnp.concatenate(squares, axis=0)
        if h > 0:
            squares = squares + jnp.concatenate([r.squares[span] for span in spans], axis=0)
        r.sq_send[n] = jnp.broadcast_to(squares, (n_tp * size, 128)).T[0:1]

    def combine_early(h):
        state = r.e_recv[h].reshape(HEAD_DIM, HEAD_DIM)
        for t in range(tiles):
            span = slice(t * TILE, (t + 1) * TILE)
            carried = dot(r.q[h, span, :], state)
            memory = r.num[h, span, :] + r.beta[h, span, :] * carried
            r.num[h, span, :] = memory
            squares = jnp.sum(memory * memory, axis=-1, keepdims=True)
            if h > 0:
                squares = squares + r.squares[span]
            r.squares[span] = squares

    def square_copies(which):
        pieces = slice(0, 1) if which == 0 else slice(1, CHUNKS)
        made = []
        for step in range(1, n_tp):
            made.append(
                remote(
                    r.sq_send.at[pieces],
                    r.sq_recv.at[step, pieces],
                    r.sq_sems.at[0, which, step],
                    r.sq_sems.at[1, which, step],
                    "tp",
                    lax.rem(tp + step, n_tp),
                )
            )
        return made

    def scales(pieces):
        for n in pieces:
            total = r.sq_send[n]
            for step in range(1, n_tp):
                total = total + r.sq_recv[step, n]
            scale = lax.rsqrt(total / (HEAD_DIM * H * n_tp) + EPS)
            scale = jnp.broadcast_to(scale, (128, n_tp * size)).T
            for b, span in enumerate(piece_spans(n)):
                r.scale[span, :] = scale[b * size : (b + 1) * size]

    for h in range(H):
        for step in range(1, quad):
            e_copy(h, step).wait()
        if h < H - 1:
            combine_early(h)
    lead_squares, rest_squares = square_copies(0), square_copies(1)
    combine(H - 1, 0)
    for copy in lead_squares:
        copy.start()
    r.sib_send[0] = memory_product(lead_theirs).astype(BF16)
    to_sibling(0)
    for n in range(1, CHUNKS):
        combine(H - 1, n)
    for copy in rest_squares:
        copy.start()
    r.lead_memory[...] = memory_product(lead_ours)
    for copy in lead_squares:
        copy.wait()
    scales([0])

    siblings[slots].wait_recv()
    siblings[0].wait_recv()
    r.link_send[0] = (
        (r.lead_memory[...] + r.sib_recv[0].astype(F32)) * r.scale[lead_ours, 0:1]
        + r.lead_pool[...]
        + r.sib_recv[slots].astype(F32)
    ).astype(BF16)
    to_chip(0, jobs[0][2])

    def send_on(job):
        j, n, target, slot = job
        if j == chips:
            return
        siblings[slot].wait_recv()
        r.link_send[slot] = (r.own[slot].astype(F32) + r.sib_recv[slot].astype(F32)).astype(BF16)
        to_chip(slot, target)

    for copy in rest_squares:
        copy.wait()
    scales(range(1, CHUNKS))
    for index, (j, n, target, slot) in enumerate(jobs):
        if index == 0:
            continue
        if j == chips and n == 0:
            gates_of(chip)
            pool_of(chip)
        r.sib_send[slot] = finish(chunk_rows(target, 1 - core, n))
        to_sibling(slot)
        r.own[slot] = finish(chunk_rows(target, core, n))
        if index > 1:
            send_on(jobs[index - 1])
    outs = []
    for n in range(CHUNKS):
        slot = (chips - 1) * CHUNKS + n
        siblings[slot].wait_recv()
        total = r.own[slot].astype(F32) + r.sib_recv[slot].astype(F32)
        for j in range(1, chips):
            other = (j - 1) * CHUNKS + n
            links[other].wait_recv()
            total = total + r.link_recv[other].astype(F32)
        scale = lax.rsqrt(jnp.mean(total * total, axis=-1, keepdims=True) + EPS)
        span = pl.ds(n * size, size)
        out_hbm[span, :] = (total * scale * r.post[...]).astype(BF16)

    @pl.when(owner != sp)
    def _():
        init_copy.wait_send()

    for h in range(H):
        @pl.when(my_quad < quads - 1)
        def _(h=h):
            t_copy(h).wait_send()

    for copy in [*siblings.values(), *links.values()]:
        copy.wait_send()
    for copy in outs:
        copy.wait()


def body(
    n_sp,
    n_tp,
    tokens,
    pre_gain,
    w_query,
    w_key,
    w_value,
    memory_output_gate_weight,
    w_input_gate,
    w_forget_gate,
    input_bias,
    forget_bias,
    forget_extra,
    initial_memory,
    initial_normal,
    memory_gain,
    w_pool_input,
    w_pool_gate,
    pool_mix,
    pool_gain,
    w_out_memory,
    w_out_pool,
    post_gain,
):
    T, D = tokens.shape
    MW = w_query.shape[1]
    PW = w_pool_input.shape[1]
    H = MW // HEAD_DIM
    G = PW // GROUP_DIM
    heads = w_input_gate.shape[1]
    part = initial_normal.shape[1]
    quad = min(QUAD, n_sp)
    rows_own = HEAD_DIM // quad
    chips = n_tp // 2
    block = T // n_tp
    slots = chips * CHUNKS
    size = block // CHUNKS
    hbm = pl.BlockSpec(memory_space=pl.ANY)
    V = pltpu.VMEM
    dma = pltpu.SemaphoreType.DMA
    scratch = dict(
        tokens=V((T, D), BF16),
        gain=V((1, D), F32),
        wq=V((D, MW), BF16),
        wk=V((D, MW), BF16),
        wv=V((D, MW), BF16),
        wg=V((D, MW), BF16),
        w_in=V((heads, D), BF16),
        w_forget=V((heads, D), BF16),
        b_in=V((1, heads), F32),
        b_forget=V((1, heads), F32),
        extra=V((H, T), F32),
        normal=V((H, part), F32),
        mem_gain=V((1, MW), F32),
        wpi=V((D, PW), BF16),
        wpg=V((D, PW), BF16),
        mix=V((G, GROUP_DIM, GROUP_DIM), BF16),
        pool_gain=V((1, PW), F32),
        wom=V((MW, D), BF16),
        wop=V((PW, D), BF16),
        post=V((1, D), F32),
        normed=V((T, D), BF16),
        q=V((H, T, HEAD_DIM), BF16),
        k=V((H, T, HEAD_DIM), BF16),
        v=V((H, T, HEAD_DIM), BF16),
        gate=V((H, T, HEAD_DIM), F32),
        pgate=V((T, PW), F32),
        ext=V((T + WIDEST, PW), BF16),
        pool=V((T, PW), BF16),
        rows=V((128, T), F32),
        cols=V((T, 128), F32),
        num=V((H, T, HEAD_DIM), F32),
        beta=V((H, T, 1), F32),
        gates_w=V((128, D), BF16),
        gates_b=V((1, 128), F32),
        raw=V((128, T), F32),
        start=V((8, HEAD_DIM), F32),
        enter=V((2 * H, HEAD_DIM), F32),
        m=V((H * (n_sp + 1), HEAD_DIM), F32),
        init=V((H, rows_own, HEAD_DIM), F32),
        state=V((H, rows_own, HEAD_DIM), F32),
        a_send=V((H, 4, HEAD_DIM), F32),
        a_recv=V((n_sp, H, 4, HEAD_DIM), F32),
        s_send=V((H, quad, rows_own, HEAD_DIM), BF16),
        s_recv=V((H, quad, rows_own, HEAD_DIM), BF16),
        e_send=V((H, quad, rows_own, HEAD_DIM), BF16),
        e_recv=V((H, quad, rows_own, HEAD_DIM), BF16),
        t_send=V((H, rows_own, HEAD_DIM), BF16),
        t_recv=V((H, rows_own, HEAD_DIM), BF16),
        squares=V((T, 1), F32),
        sq_send=V((CHUNKS, 1, T // CHUNKS), F32),
        sq_recv=V((n_tp, CHUNKS, 1, T // CHUNKS), F32),
        lead_pool=V((size, D), F32),
        lead_memory=V((size, D), F32),
        scale=V((T, 128), F32),
        sib_send=V((slots + 1, size, D), BF16),
        sib_recv=V((slots + 1, size, D), BF16),
        own=V((slots, size, D), BF16),
        link_send=V((slots, size, D), BF16),
        link_recv=V((slots, size, D), BF16),
        local_sem=dma((INPUTS + T // TILE + 2 * H,)),
        init_sems=dma((n_sp // quad + 1,)),
        a_sems=dma((2, H, n_sp)),
        s_sems=dma((2, H, quad)),
        e_sems=dma((2, H, quad)),
        t_sems=dma((2, H)),
        halo_sems=dma((2,)),
        sq_sems=dma((2, 2, n_tp)),
        sib_sems=dma((2, slots + 1)),
        link_sems=dma((2, slots)),
    )
    return pl.pallas_call(
        functools.partial(kernel, n_sp, n_tp, tuple(scratch)),
        out_shape=pltpu.VMEM((block, D), BF16),
        in_specs=[hbm] * INPUTS,
        out_specs=pl.BlockSpec(memory_space=pltpu.VMEM),
        scratch_shapes=list(scratch.values()),
        compiler_params=pltpu.CompilerParams(
            collective_id=0, has_side_effects=True, vmem_limit_bytes=60 * 1024 * 1024
        ),
    )(
        tokens,
        pre_gain[None],
        w_query,
        w_key,
        w_value,
        memory_output_gate_weight,
        w_input_gate.T,
        w_forget_gate.T,
        input_bias[None],
        forget_bias[None],
        forget_extra.T,
        initial_memory,
        initial_normal,
        memory_gain[None],
        w_pool_input,
        w_pool_gate,
        pool_mix,
        pool_gain[None],
        w_out_memory,
        w_out_pool,
        post_gain[None],
    )


def solution(mesh):
    in_specs = (
        P("sp", None),
        P(),
        P(None, "tp"),
        P(None, "tp"),
        P(None, "tp"),
        P(None, "tp"),
        P(),
        P(),
        P(),
        P(),
        P("sp", "tp"),
        P("tp", "sp", None),
        P("tp", "sp"),
        P(),
        P(None, "tp"),
        P(None, "tp"),
        P(),
        P(),
        P("tp", None),
        P("tp", None),
        P(),
    )
    out_specs = P(("sp", "tp"), None)
    sizes = dict(mesh.shape)
    run = functools.partial(body, sizes["sp"], sizes["tp"])
    return jax.shard_map(run, mesh=mesh, in_specs=in_specs, out_specs=out_specs, check_vma=False)
```

```python
import functools
import types

import jax
import jax.numpy as jnp
from jax import lax
from jax.experimental import pallas as pl
from jax.experimental.pallas import tpu as pltpu
from jax.sharding import PartitionSpec as P

HEAD_DIM = 256
GROUP_DIM = 128
WIDEST = 256
TILE = 256
SHARES = (2, 1, 1, 2, 2)
QUAD = 4
SUB = 64
EPS = 1e-06
FLOOR = -1e30
F32 = jnp.float32
BF16 = jnp.bfloat16
MESH = pl.DeviceIdType.MESH
INPUTS = 21


def dot(a, b):
    return jnp.dot(a, b, preferred_element_type=F32)


def dot_t(a, b):
    return lax.dot_general(a, b, (((1,), (1,)), ((), ())), preferred_element_type=F32)


def silu(x):
    return x / (1.0 + jnp.exp(-x))


def kernel(n_sp, n_tp, names, *refs):
    (
        tokens_hbm,
        gain_hbm,
        wq_hbm,
        wk_hbm,
        wv_hbm,
        wg_hbm,
        w_in_hbm,
        w_forget_hbm,
        b_in_hbm,
        b_forget_hbm,
        extra_hbm,
        init_hbm,
        normal_hbm,
        mem_gain_hbm,
        wpi_hbm,
        wpg_hbm,
        mix_hbm,
        pool_gain_hbm,
        wom_hbm,
        wop_hbm,
        post_hbm,
    ) = refs[:INPUTS]
    out_ref = refs[INPUTS]
    r = types.SimpleNamespace(**dict(zip(names, refs[INPUTS + 1 :])))
    T, D = r.tokens.shape
    H = r.q.shape[0]
    G = r.mix.shape[0]
    heads = r.w_in.shape[0]
    sp = lax.axis_index("sp")
    tp = lax.axis_index("tp")
    head_scale = HEAD_DIM ** (-0.5)
    tiles = T // TILE
    quad = r.e_recv.shape[1]
    rows_own = HEAD_DIM // quad
    quads = n_sp // quad
    my_quad, my_slot = sp // quad, lax.rem(sp, quad)
    part = HEAD_DIM // n_sp

    mem_lanes = pl.ds(pl.multiple_of(tp * H * HEAD_DIM, HEAD_DIM), H * HEAD_DIM)
    pool_lanes = pl.ds(pl.multiple_of(tp * G * GROUP_DIM, GROUP_DIM), G * GROUP_DIM)
    loads = {}

    def load(name, src, dst, slot=None):
        slot = len(loads) if slot is None else slot
        loads[name] = pltpu.make_async_copy(src, dst, r.local_sem.at[slot])
        loads[name].start()

    load("gain", gain_hbm, r.gain)

    def load_tokens(t):
        span = pl.ds(t * TILE, TILE)
        load(("tokens", t), tokens_hbm.at[span], r.tokens.at[span])

    def load_head(name, source, target, h):
        lanes = pl.ds(h * HEAD_DIM, HEAD_DIM)
        load((name, h), source.at[:, lanes], target.at[:, lanes])

    for t in range(tiles // 2):
        load_tokens(t)
    load("w_in", w_in_hbm, r.w_in)
    load("w_forget", w_forget_hbm, r.w_forget)
    load("b_in", b_in_hbm, r.b_in)
    load("b_forget", b_forget_hbm, r.b_forget)
    load_head("wk", wk_hbm, r.wk, 0)
    for t in range(tiles // 2, tiles):
        load_tokens(t)
    load_head("wv", wv_hbm, r.wv, 0)
    load("extra", extra_hbm, r.extra)
    load("normal", normal_hbm, r.normal)
    for h in range(1, H):
        load_head("wk", wk_hbm, r.wk, h)
        load_head("wv", wv_hbm, r.wv, h)
    load("wpi", wpi_hbm, r.wpi)
    load("wq", wq_hbm, r.wq)

    r.ext[0:WIDEST, :] = jnp.zeros((WIDEST, r.ext.shape[1]), BF16)
    barrier = pltpu.get_barrier_semaphore()
    for step in range(1, n_sp):
        pl.semaphore_signal(
            barrier, inc=1, device_id={"sp": lax.rem(sp + step, n_sp)}, device_id_type=MESH
        )
    for step in range(1, n_tp):
        pl.semaphore_signal(
            barrier, inc=1, device_id={"tp": lax.rem(tp + step, n_tp)}, device_id_type=MESH
        )

    def remote(src, dst, send_sem, recv_sem, axis, peer):
        return pltpu.make_async_remote_copy(
            src_ref=src,
            dst_ref=dst,
            send_sem=send_sem,
            recv_sem=recv_sem,
            device_id={axis: peer},
            device_id_type=MESH,
        )

    r.gates_w[...] = jnp.zeros_like(r.gates_w)
    r.gates_b[...] = jnp.zeros_like(r.gates_b)
    r.rows[...] = jnp.zeros_like(r.rows)
    r.a_send[...] = jnp.zeros_like(r.a_send)
    loads["gain"].wait()
    loads["tokens", 0].wait()

    def norm_tile(rows):
        x = r.tokens[rows, :].astype(F32)
        scale = lax.rsqrt(jnp.mean(x * x, axis=-1, keepdims=True) + EPS)
        r.normed[rows, :] = (x * scale * r.gain[...]).astype(BF16)

    def head_lanes(h):
        return slice(h * HEAD_DIM, (h + 1) * HEAD_DIM)

    def whole(ref, h):
        return lambda rows, value: ref.__setitem__((h, rows), value.astype(ref.dtype))

    def gates_product(rows):
        r.cols[rows, :] = dot_t(r.normed[rows, :], r.gates_w[...]) + r.gates_b[...]

    def product(weight, lanes, rows, store):
        store(rows, dot(r.normed[rows, :], weight[:, lanes]))

    per_owner = n_sp // quad
    owner = sp // per_owner
    turn = lax.rem(sp, per_owner)
    init_place = r.init.at[:, pl.ds(pl.multiple_of(turn * part, part), part), :]
    init_copy = remote(
        init_hbm, init_place, r.init_sems.at[per_owner], r.init_sems.at[turn], "sp", owner
    )
    init_local = pltpu.make_async_copy(init_hbm, init_place, r.init_sems.at[per_owner])

    def send_init():
        pl.semaphore_wait(barrier, n_sp - 1 + n_tp - 1)

        @pl.when(owner != sp)
        def _():
            init_copy.start()

        @pl.when(owner == sp)
        def _():
            init_local.start()

    half = tiles // 2
    for t in range(half):
        if t > 0:
            loads["tokens", t].wait()
        for sub in range(0, TILE, SUB):
            norm_tile(pl.ds(t * TILE + sub, SUB))
    for name in ("w_in", "w_forget", "b_in", "b_forget", ("wk", 0)):
        loads[name].wait()
    load("wpg", wpg_hbm, r.wpg, 0)
    load("wg", wg_hbm, r.wg, 1)
    load("mix", mix_hbm.at[pl.ds(tp * G, G)], r.mix, 2)
    load("pool_gain", pool_gain_hbm.at[:, pool_lanes], r.pool_gain, 3)
    load("mem_gain", mem_gain_hbm.at[:, mem_lanes], r.mem_gain, 4)
    load("wop", wop_hbm, r.wop, 5)
    load("wom", wom_hbm, r.wom, 6)
    load("post", post_hbm, r.post, 7)
    r.gates_w[0:heads, :] = r.w_in[...]
    r.gates_w[heads : 2 * heads, :] = r.w_forget[...]
    r.gates_b[:, 0:heads] = r.b_in[...]
    r.gates_b[:, heads : 2 * heads] = r.b_forget[...]
    def early_products(rows):
        gates_product(rows)
        product(r.wk, head_lanes(0), rows, whole(r.k, 0))

    pieces = (slice(0, half * TILE), slice(half * TILE, T))
    loads["tokens", half].wait()
    early_products(pieces[0])
    for t in range(half, tiles):
        if t > half:
            loads["tokens", t].wait()
            if t == half + 1:
                loads["wv", 0].wait()
                for part_rows in (slice(0, TILE), slice(TILE, half * TILE)):
                    product(r.wv, head_lanes(0), part_rows, whole(r.v, 0))
        for sub in range(0, TILE, SUB):
            norm_tile(pl.ds(t * TILE + sub, SUB))
    send_init()
    for name in ("extra", "normal"):
        loads[name].wait()
    for h in range(1, H):
        loads["wk", h].wait()
        loads["wv", h].wait()
    early_products(pieces[1])
    for start in (half * TILE, half * TILE + TILE):
        product(r.wv, head_lanes(0), slice(start, start + TILE), whole(r.v, 0))

    tri = (
        lax.broadcasted_iota(jnp.int32, (TILE, TILE), 0)
        <= lax.broadcasted_iota(jnp.int32, (TILE, TILE), 1)
    ).astype(F32)
    spare = [jnp.zeros((8 - H, TILE), F32)]
    log_keeps = []
    for t in range(tiles):
        span = pl.ds(t * TILE, TILE)
        r.raw[:, span] = r.cols[span, :].T
        own_rows = [r.raw[pl.ds(heads + tp * H + h, 1), span] for h in range(H)]
        added = [r.extra[h : h + 1, span] for h in range(H)]
        raw = jnp.concatenate(own_rows + spare, axis=0)
        log_keep = jnp.minimum(raw, 0.0) - jnp.log1p(jnp.exp(-jnp.abs(raw)))
        log_keeps.append(log_keep + jnp.concatenate(added + spare, axis=0))
    runs = jnp.dot(
        jnp.concatenate(log_keeps, axis=0),
        tri,
        preferred_element_type=F32,
        precision=lax.Precision.HIGHEST,
    )
    last = [runs[8 * t : 8 * t + 8, TILE - 1 : TILE] for t in range(tiles)]
    carry = jnp.zeros((8, 1), F32)
    for t in range(tiles):
        span = pl.ds(t * TILE, TILE)
        run = carry + runs[8 * t : 8 * t + 8]
        carry = carry + last[t]
        for h in range(H):
            keep = run[h : h + 1]
            r.rows[h : h + 1, span] = r.raw[pl.ds(tp * H + h, 1), span] - keep
            r.rows[H + h : H + h + 1, span] = keep
    for t in range(tiles):
        span = pl.ds(t * TILE, TILE)
        r.cols[span, :] = r.rows[:, span].T

    def a_copy(h, step):
        peer = lax.rem(sp + step, n_sp)
        return remote(
            r.a_send.at[h], r.a_recv.at[sp, h], r.a_sems.at[0, h], r.a_sems.at[1, h], "sp", peer
        )

    def s_copy(h, step):
        peer = lax.rem(my_slot + step, quad)
        return remote(
            r.s_send.at[h, peer],
            r.s_recv.at[h, my_slot],
            r.s_sems.at[0, h],
            r.s_sems.at[1, h],
            "sp",
            my_quad * quad + peer,
        )

    def e_copy(h, step):
        peer = lax.rem(my_slot + step, quad)
        return remote(
            r.e_send.at[h, peer],
            r.e_recv.at[h, my_slot],
            r.e_sems.at[0, h],
            r.e_sems.at[1, h],
            "sp",
            my_quad * quad + peer,
        )

    def all_of(ref, sems, axis="sp"):
        peer = lax.rem(sp + 1, n_sp) if axis == "sp" else lax.rem(tp + 1, n_tp)
        return remote(ref, ref, sems[0], sems[1], axis, peer)

    def t_copy(h):
        return remote(
            r.t_send.at[h],
            r.t_recv.at[h],
            r.t_sems.at[0, h],
            r.t_sems.at[1, h],
            "sp",
            lax.rem(sp + quad, n_sp),
        )

    for h in range(H):
        if h > 0:
            for rows in pieces:
                product(r.wk, head_lanes(h), rows, whole(r.k, h))
            for rows in pieces:
                product(r.wv, head_lanes(h), rows, whole(r.v, h))
        a_max = jnp.max(r.rows[h : h + 1, :], axis=-1, keepdims=True)
        total = r.rows[H + h : H + h + 1, T - 1 : T]
        state = jnp.zeros((HEAD_DIM, HEAD_DIM), F32)
        normal = jnp.zeros((1, HEAD_DIM), F32)
        for t in range(tiles):
            span = pl.ds(t * TILE, TILE)
            weight = jnp.exp(r.cols[span, h : h + 1] - a_max)
            kw = weight * r.k[h, span, :].astype(F32)
            normal = normal + jnp.sum(kw, axis=0, keepdims=True)
            state = state + lax.dot_general(
                kw.astype(BF16),
                r.v[h, span, :],
                (((0,), (0,)), ((), ())),
                preferred_element_type=F32,
            )
        r.s_send[h] = state.reshape(quad, rows_own, HEAD_DIM).astype(BF16)
        r.a_send[h, 0:1, :] = jnp.broadcast_to(total + a_max, (1, HEAD_DIM))
        r.a_send[h, 1:2, :] = jnp.broadcast_to(total, (1, HEAD_DIM))
        r.a_send[h, 2:3, :] = normal
        r.a_send[h, 3:4, 0:part] = r.normal[h : h + 1, :]
        for step in range(1, n_sp):
            a_copy(h, step).start()
        for step in range(1, quad):
            s_copy(h, step).start()
        r.s_recv[h, my_slot] = r.s_send[h, my_slot]
        r.a_recv[sp, h] = r.a_send[h]

    def m_row(h, j):
        return pl.ds(h * (n_sp + 1) + j, 1)

    def chain(h):
        all_of(r.a_recv.at[pl.ds(0, n_sp - 1), h], (r.a_sems.at[0, h], r.a_sems.at[1, h])).wait()
        for j in range(n_sp):
            r.start[h : h + 1, j * part : (j + 1) * part] = r.a_recv[j, h, 3:4, 0:part]
        normal = r.start[h : h + 1, :]
        stab = jnp.zeros((1, HEAD_DIM), F32)
        my_stab, my_normal = stab, normal
        for j in range(n_sp):
            r.m[m_row(h, j), :] = stab
            if j > 0:
                my_stab = jnp.where(sp == j, stab, my_stab)
                my_normal = jnp.where(sp == j, normal, my_normal)
            late = r.a_recv[j, h, 0:1, :]
            keep = r.a_recv[j, h, 1:2, :]
            joint = jnp.maximum(late, keep + stab)
            normal = normal * jnp.exp(keep + stab - joint) + r.a_recv[j, h, 2:3, :] * jnp.exp(
                late - joint
            )
            stab = joint
        r.m[m_row(h, n_sp), :] = stab
        r.enter[h : h + 1, :] = my_stab
        r.enter[H + h : H + h + 1, :] = my_normal

    def spread(h):
        state = r.state[h]
        for i in range(quad):
            j = my_quad * quad + i
            r.e_send[h, i] = state.astype(BF16)
            stab, joint = r.m[m_row(h, j), :], r.m[m_row(h, j + 1), :]
            late = r.a_recv[j, h, 0:1, :]
            keep = r.a_recv[j, h, 1:2, :]
            state = state * jnp.exp(keep + stab - joint) + r.s_recv[h, i].astype(F32) * jnp.exp(
                late - joint
            )
        r.t_send[h] = state.astype(BF16)

        @pl.when(my_quad < quads - 1)
        def _():
            t_copy(h).start()

        for step in range(1, quad):
            e_copy(h, step).start()
        r.e_recv[h, my_slot] = r.e_send[h, my_slot]

    def gathered(h):
        chain(h)
        all_of(r.s_recv.at[h, pl.ds(0, quad - 1)], (r.s_sems.at[0, h], r.s_sems.at[1, h])).wait()

        @pl.when(my_quad == 0)
        def _():
            if h == 0:
                for turn_in in range(per_owner):
                    source = sp * per_owner + turn_in

                    @pl.when(source != sp)
                    def _():
                        init_copy_from(turn_in).wait_recv()

                @pl.when(owner == sp)
                def _():
                    init_local.wait()

            r.state[h] = r.init[h]
            spread(h)

    def init_copy_from(turn_in):
        place = r.init.at[:, pl.ds(turn_in * part, part), :]
        return remote(init_hbm, place, r.init_sems.at[per_owner], r.init_sems.at[turn_in], "sp", owner)

    def carried_on(h):
        @pl.when(my_quad > 0)
        def _():
            t_copy(h).wait_recv()
            r.state[h] = r.t_recv[h].astype(F32)
            spread(h)

    loads["wpi"].wait()
    loads["wq"].wait()

    def store_pool(rows, value):
        r.ext[WIDEST + rows.start : WIDEST + rows.stop, :] = value.astype(BF16)

    for rows in pieces:
        product(r.wpi, slice(None), rows, store_pool)

    def halo_copy(member):
        width = min(WIDEST, max(16, 2 ** (G * (member + 1))))
        return remote(
            r.ext.at[pl.ds(T + WIDEST - width, width)],
            r.ext.at[pl.ds(WIDEST - width, width)],
            r.halo_sems.at[0],
            r.halo_sems.at[1],
            "sp",
            lax.rem(sp + 1, n_sp),
        )

    for member in range(n_tp):

        @pl.when((tp == member) & (sp < n_sp - 1))
        def _(member=member):
            halo_copy(member).start()


    def query_to(h):
        def store(rows, value):
            r.q[h, rows, :] = value.astype(BF16) * head_scale

        return store

    for rows in pieces:
        product(r.wq, head_lanes(0), rows, query_to(0))
    gathered(0)
    for h in range(1, H):
        for rows in pieces:
            product(r.wq, head_lanes(h), rows, query_to(h))
    for name in ("wg", "mem_gain", "wpg", "pool_gain", "mix", "wop", "wom", "post"):
        loads[name].wait()
    chips = n_tp // 2
    chip, core = tp // 2, lax.rem(tp, 2)
    sibling = chip * 2 + 1 - core
    block = T // n_tp
    segment = 2 * block
    unit = block // sum(SHARES)
    chunks = []
    for share in SHARES:
        begin = chunks[-1][0] + chunks[-1][1] if chunks else 0
        chunks.append((begin, share * unit))
    count = len(chunks)
    extra_slot = chips * count
    lead = chunks[0][1]

    def chunk_rows(target, which, n):
        begin, size = chunks[n]
        return pl.ds(pl.multiple_of((target * 2 + which) * block + begin, unit), size)

    first_target = lax.rem(chip + 1, chips)
    lead_theirs = chunk_rows(first_target, 1 - core, 0)
    lead_ours = chunk_rows(first_target, core, 0)

    def gate_to(h):
        def store(rows, value):
            r.gate[h, rows, :] = r.mem_gain[:, head_lanes(h)] * silu(value)

        return store

    def store_gate(rows, value):
        r.pgate[rows, :] = r.pool_gain[...] * silu(value)

    def gates_of(target):
        start = pl.multiple_of(target * segment, segment)
        for h in range(H):
            product(r.wg, head_lanes(h), pl.ds(start, segment), gate_to(h))
        for piece in range(2):
            rows = pl.ds(pl.multiple_of(start + piece * block, block), block)
            product(r.wpg, slice(None), rows, store_gate)

    def lead_pair(ref):
        return jnp.concatenate([ref[lead_theirs, :], ref[lead_ours, :]], axis=0)

    def pool_rows(start, size):
        for g in range(G):
            window = jnp.left_shift(2, tp * G + g)
            offset = (
                lax.broadcasted_iota(jnp.int32, (size, size + WIDEST), 0)
                + WIDEST
                - lax.broadcasted_iota(jnp.int32, (size, size + WIDEST), 1)
            )
            band = jnp.where((offset >= 0) & (offset < window), 1.0, 0.0).astype(BF16)
            lanes = slice(g * GROUP_DIM, (g + 1) * GROUP_DIM)
            span = pl.ds(start, size)
            here = r.ext[pl.ds(pl.multiple_of(start + WIDEST, unit), size), lanes]
            before = r.ext[pl.ds(start, WIDEST), lanes]
            sums = dot(band[:, :WIDEST], before) + dot(band[:, WIDEST:], here)
            position = lax.broadcasted_iota(jnp.int32, (size, 1), 0) + (sp * T + start + 1)
            counts = jnp.minimum(position, window).astype(F32)
            pooled = (sums / counts - here.astype(F32)).astype(BF16)
            r.pool[span, lanes] = (dot(pooled, r.mix[g]) * r.pgate[span, lanes]).astype(BF16)

    def pool_of(target):
        for piece in range(segment // TILE):
            pool_rows(pl.multiple_of(target * segment + piece * TILE, TILE), TILE)

    value = dot(lead_pair(r.normed), r.wpg[...])
    store_gate(lead_theirs, value[:lead])
    store_gate(lead_ours, value[lead:])
    value = dot(lead_pair(r.normed), r.wg[...])
    for h in range(H):
        gate_to(h)(lead_theirs, value[:lead, head_lanes(h)])
        gate_to(h)(lead_ours, value[lead:, head_lanes(h)])
    for h in range(1, H):
        gathered(h)
    for member in range(n_tp):

        @pl.when((tp == member) & (sp > 0))
        def _(member=member):
            halo_copy(member).wait_recv()

    for which in (1 - core, core):
        pool_rows(pl.multiple_of((first_target * 2 + which) * block, block), lead)
    def memory_product(rows):
        parts = [(r.num[h, rows, :] * r.gate[h, rows, :]).astype(BF16) for h in range(H)]
        return dot(parts[0] if H == 1 else jnp.concatenate(parts, axis=1), r.wom[...])

    def finish(rows):
        pool = dot(r.pool[rows, :], r.wop[...])
        return (memory_product(rows) * r.scale[rows, 0:1] + pool).astype(BF16)

    jobs = []
    for j in range(1, chips + 1):
        for n in range(count):
            jobs.append((j, n, lax.rem(chip + j, chips)))

    siblings, links = {}, {}

    def place(j, n):
        if n < 0:
            return pl.ds(chips * block, lead)
        begin, size = chunks[n]
        return pl.ds((j - 1) * block + begin, size)

    def to_sibling(j, n):
        slot = extra_slot if n < 0 else (j - 1) * count + n
        rows = place(j, n)
        siblings[j, n] = remote(
            r.sib_send.at[rows],
            r.sib_recv.at[rows],
            r.sib_sems.at[extra_slot + 1],
            r.sib_sems.at[slot],
            "tp",
            sibling,
        )
        siblings[j, n].start()

    def to_chip(j, n, target):
        slot = extra_slot - count if n < 0 else (j - 1) * count + n
        rows = place(j, n)
        links[j, n] = remote(
            r.link_send.at[rows],
            r.link_recv.at[rows],
            r.link_sems.at[extra_slot - count + 1],
            r.link_sems.at[slot],
            "tp",
            target * 2 + core,
        )
        links[j, n].start()

    r.sib_send[place(1, -1), :] = dot(r.pool[lead_theirs, :], r.wop[...]).astype(BF16)
    to_sibling(1, -1)
    r.lead[...] = dot(r.pool[lead_ours, :], r.wop[...])

    def pass_on(j, n, target):
        siblings[j, n].wait_recv()
        rows = place(j, n)
        mine = r.lead[...] if (j, max(n, 0)) == (1, 0) else r.own[rows, :].astype(F32)
        r.link_send[rows, :] = (mine + r.sib_recv[rows, :].astype(F32)).astype(BF16)
        to_chip(j, n, target)

    carried_on(0)
    diag_mask = lax.broadcasted_iota(jnp.int32, (TILE, TILE), 0) >= lax.broadcasted_iota(
        jnp.int32, (TILE, TILE), 1
    )

    def attend(h):
        enter_max = r.enter[h : h + 1, 0:1]
        enter_normal = r.enter[H + h : H + h + 1, :]
        for t in range(tiles):
            span = pl.ds(t * TILE, TILE)
            queries = r.q[h, span, :]
            near = jnp.where(diag_mask, r.rows[h : h + 1, span], FLOOR)
            top = jnp.max(near, axis=-1, keepdims=True)
            if t > 0:
                far = r.rows[h : h + 1, 0 : t * TILE]
                top = jnp.maximum(top, jnp.max(far, axis=-1, keepdims=True))
            weights = jnp.exp(near - top) * dot_t(queries, r.k[h, span, :])
            den = jnp.sum(weights, axis=-1, keepdims=True)
            num = dot(weights.astype(BF16), r.v[h, span, :])
            if t > 0:
                weights = jnp.exp(far - top) * dot_t(queries, r.k[h, 0 : t * TILE, :])
                den = den + jnp.sum(weights, axis=-1, keepdims=True)
                num = num + dot(weights.astype(BF16), r.v[h, 0 : t * TILE, :])
            keep = r.cols[span, H + h : H + h + 1]
            row_max = keep + top
            carried = keep + enter_max
            joint = jnp.maximum(row_max, carried)
            local_weight = jnp.exp(row_max - joint)
            carry_weight = jnp.exp(carried - joint)
            den = den * local_weight + carry_weight * jnp.sum(
                queries.astype(F32) * enter_normal, axis=-1, keepdims=True
            )
            bound = jnp.maximum(jnp.abs(den), jnp.exp(-joint))
            r.num[h, span, :] = num * (local_weight / bound)
            r.beta[h, span, :] = carry_weight / bound

    attend(0)
    pass_on(1, -1, first_target)
    for h in range(1, H):
        carried_on(h)

    for h in range(1, H):
        attend(h)
    def combine(h):
        state = r.e_recv[h].reshape(HEAD_DIM, HEAD_DIM)
        for t in range(tiles):
            span = slice(t * TILE, (t + 1) * TILE)
            carried = dot(r.q[h, span, :], state)
            memory = r.num[h, span, :] + r.beta[h, span, :] * carried
            r.num[h, span, :] = memory
            squares = jnp.sum(memory * memory, axis=-1, keepdims=True)
            if h > 0:
                squares = squares + r.squares[span]
            if h < H - 1:
                r.squares[span] = squares
            else:
                r.sq_send[:, span] = jnp.broadcast_to(squares, (TILE, 128)).T[0:1]

    for h in range(H):
        all_of(r.e_recv.at[h, pl.ds(0, quad - 1)], (r.e_sems.at[0, h], r.e_sems.at[1, h])).wait()
        combine(h)
    third = []
    for step in range(1, n_tp):
        third.append(
            remote(
                r.sq_send,
                r.sq_recv.at[step],
                r.sq_sems.at[0],
                r.sq_sems.at[1],
                "tp",
                lax.rem(tp + step, n_tp),
            )
        )
    for copy in third:
        copy.start()
    r.sib_send[place(1, 0), :] = memory_product(lead_theirs).astype(BF16)
    to_sibling(1, 0)
    r.lead[...] = memory_product(lead_ours)
    pass_on(1, 0, first_target)
    for j in range(1, chips):
        gates_of(lax.rem(chip + j, chips))
        pool_of(lax.rem(chip + j, chips))
    all_of(r.sq_recv.at[pl.ds(0, n_tp - 1)], (r.sq_sems.at[0], r.sq_sems.at[1]), "tp").wait()
    for t in range(tiles):
        span = pl.ds(t * TILE, TILE)
        total = r.sq_send[0:1, span]
        for step in range(1, n_tp):
            total = total + r.sq_recv[step, 0:1, span]
        scale = lax.rsqrt(total / (HEAD_DIM * H * n_tp) + EPS)
        r.scale[span, :] = jnp.broadcast_to(scale, (128, TILE)).T

    for index, (j, n, target) in enumerate(jobs):
        if index == 0:
            continue
        if j == chips and n == 0:
            gates_of(chip)
            pool_of(chip)
        r.sib_send[place(j, n), :] = finish(chunk_rows(target, 1 - core, n))
        to_sibling(j, n)
        r.own[place(j, n), :] = finish(chunk_rows(target, core, n))
        if index == 1 and j < chips:
            pass_on(j, n, target)
        elif index > 2 and jobs[index - 1][0] < chips:
            pass_on(*jobs[index - 1])
    own_scale = r.scale.at[pl.ds(pl.multiple_of(tp * block, block), lead)]
    for n in range(count):
        siblings[chips, n].wait_recv()
        begin, size = chunks[n]
        total = r.own[place(chips, n), :].astype(F32) + r.sib_recv[place(chips, n), :].astype(F32)
        for j in range(1, chips):
            links[j, n].wait_recv()
            came = r.link_recv[place(j, n), :].astype(F32)
            if (j, n) == (1, 0):
                links[1, -1].wait_recv()
                came = came * own_scale[:, 0:1] + r.link_recv[place(1, -1), :].astype(F32)
            total = total + came
        scale = lax.rsqrt(jnp.mean(total * total, axis=-1, keepdims=True) + EPS)
        out_ref[begin : begin + size, :] = (total * scale * r.post[...]).astype(BF16)
    for member in range(n_tp):

        @pl.when((tp == member) & (sp < n_sp - 1))
        def _(member=member):
            halo_copy(member).wait_send()


    @pl.when(owner != sp)
    def _():
        init_copy.wait_send()

    for h in range(H):
        @pl.when(my_quad < quads - 1)
        def _(h=h):
            t_copy(h).wait_send()

    sent = r.sib_send.at[pl.ds(0, chips * block + lead)]
    all_of(sent, (r.sib_sems.at[extra_slot + 1], r.sib_sems.at[0]), "tp").wait_send()
    sent = r.link_send.at[pl.ds(0, (chips - 1) * block + lead)]
    all_of(sent, (r.link_sems.at[extra_slot - count + 1], r.link_sems.at[0]), "tp").wait_send()


def body(
    n_sp,
    n_tp,
    tokens,
    pre_gain,
    w_query,
    w_key,
    w_value,
    memory_output_gate_weight,
    w_input_gate,
    w_forget_gate,
    input_bias,
    forget_bias,
    forget_extra,
    initial_memory,
    initial_normal,
    memory_gain,
    w_pool_input,
    w_pool_gate,
    pool_mix,
    pool_gain,
    w_out_memory,
    w_out_pool,
    post_gain,
):
    T, D = tokens.shape
    MW = w_query.shape[1]
    PW = w_pool_input.shape[1]
    H = MW // HEAD_DIM
    G = PW // GROUP_DIM
    heads = w_input_gate.shape[1]
    part = initial_normal.shape[1]
    quad = min(QUAD, n_sp)
    rows_own = HEAD_DIM // quad
    chips = n_tp // 2
    block = T // n_tp
    slots = chips * len(SHARES)
    lead = block // sum(SHARES) * SHARES[0]
    hbm = pl.BlockSpec(memory_space=pl.ANY)
    V = pltpu.VMEM
    dma = pltpu.SemaphoreType.DMA
    scratch = dict(
        tokens=V((T, D), BF16),
        gain=V((1, D), F32),
        wq=V((D, MW), BF16),
        wk=V((D, MW), BF16),
        wv=V((D, MW), BF16),
        wg=V((D, MW), BF16),
        w_in=V((heads, D), BF16),
        w_forget=V((heads, D), BF16),
        b_in=V((1, heads), F32),
        b_forget=V((1, heads), F32),
        extra=V((H, T), F32),
        normal=V((H, part), F32),
        mem_gain=V((1, MW), F32),
        wpi=V((D, PW), BF16),
        wpg=V((D, PW), BF16),
        mix=V((G, GROUP_DIM, GROUP_DIM), BF16),
        pool_gain=V((1, PW), F32),
        wom=V((MW, D), BF16),
        wop=V((PW, D), BF16),
        post=V((1, D), F32),
        normed=V((T, D), BF16),
        q=V((H, T, HEAD_DIM), BF16),
        k=V((H, T, HEAD_DIM), BF16),
        v=V((H, T, HEAD_DIM), BF16),
        gate=V((H, T, HEAD_DIM), F32),
        pgate=V((T, PW), F32),
        ext=V((T + WIDEST, PW), BF16),
        pool=V((T, PW), BF16),
        rows=V((128, T), F32),
        cols=V((T, 128), F32),
        num=V((H, T, HEAD_DIM), F32),
        beta=V((H, T, 1), F32),
        gates_w=V((128, D), BF16),
        gates_b=V((1, 128), F32),
        raw=V((128, T), F32),
        start=V((8, HEAD_DIM), F32),
        enter=V((2 * H, HEAD_DIM), F32),
        m=V((H * (n_sp + 1), HEAD_DIM), F32),
        init=V((H, rows_own, HEAD_DIM), F32),
        state=V((H, rows_own, HEAD_DIM), F32),
        a_send=V((H, 4, HEAD_DIM), F32),
        a_recv=V((n_sp, H, 4, HEAD_DIM), F32),
        s_send=V((H, quad, rows_own, HEAD_DIM), BF16),
        s_recv=V((H, quad, rows_own, HEAD_DIM), BF16),
        e_send=V((H, quad, rows_own, HEAD_DIM), BF16),
        e_recv=V((H, quad, rows_own, HEAD_DIM), BF16),
        t_send=V((H, rows_own, HEAD_DIM), BF16),
        t_recv=V((H, rows_own, HEAD_DIM), BF16),
        squares=V((T, 1), F32),
        sq_send=V((1, T), F32),
        sq_recv=V((n_tp, 1, T), F32),
        lead=V((lead, D), F32),
        scale=V((T, 128), F32),
        sib_send=V((chips * block + lead, D), BF16),
        sib_recv=V((chips * block + lead, D), BF16),
        own=V((chips * block, D), BF16),
        link_send=V((chips * block + lead, D), BF16),
        link_recv=V((chips * block + lead, D), BF16),
        local_sem=dma((INPUTS - 8 + T // TILE + 2 * H,)),
        init_sems=dma((n_sp // quad + 1,)),
        a_sems=dma((2, H)),
        s_sems=dma((2, H)),
        e_sems=dma((2, H)),
        t_sems=dma((2, H)),
        halo_sems=dma((2,)),
        sq_sems=dma((2,)),
        sib_sems=dma((slots + 2,)),
        link_sems=dma((slots - len(SHARES) + 2,)),
    )
    return pl.pallas_call(
        functools.partial(kernel, n_sp, n_tp, tuple(scratch)),
        out_shape=pltpu.VMEM((block, D), BF16),
        in_specs=[hbm] * INPUTS,
        out_specs=pl.BlockSpec(memory_space=pltpu.VMEM),
        scratch_shapes=list(scratch.values()),
        compiler_params=pltpu.CompilerParams(
            collective_id=0, has_side_effects=True, vmem_limit_bytes=60 * 1024 * 1024
        ),
    )(
        tokens,
        pre_gain[None],
        w_query,
        w_key,
        w_value,
        memory_output_gate_weight,
        w_input_gate.T,
        w_forget_gate.T,
        input_bias[None],
        forget_bias[None],
        forget_extra.T,
        initial_memory,
        initial_normal,
        memory_gain[None],
        w_pool_input,
        w_pool_gate,
        pool_mix,
        pool_gain[None],
        w_out_memory,
        w_out_pool,
        post_gain[None],
    )


def solution(mesh):
    in_specs = (
        P("sp", None),
        P(),
        P(None, "tp"),
        P(None, "tp"),
        P(None, "tp"),
        P(None, "tp"),
        P(),
        P(),
        P(),
        P(),
        P("sp", "tp"),
        P("tp", "sp", None),
        P("tp", "sp"),
        P(),
        P(None, "tp"),
        P(None, "tp"),
        P(),
        P(),
        P("tp", None),
        P("tp", None),
        P(),
    )
    out_specs = P(("sp", "tp"), None)
    sizes = dict(mesh.shape)
    run = functools.partial(body, sizes["sp"], sizes["tp"])
    return jax.shard_map(run, mesh=mesh, in_specs=in_specs, out_specs=out_specs, check_vma=False)
```

```python
import functools
import types

import jax
import jax.numpy as jnp
from jax import lax
from jax.experimental import pallas as pl
from jax.experimental.pallas import tpu as pltpu
from jax.sharding import PartitionSpec as P

HEAD_DIM = 256
GROUP_DIM = 128
WIDEST = 256
TILE = 256
SHARES = (2, 1, 1, 2, 2)
QUAD = 4
SUB = 64
EPS = 1e-06
FLOOR = -1e30
F32 = jnp.float32
BF16 = jnp.bfloat16
MESH = pl.DeviceIdType.MESH
INPUTS = 21


def dot(a, b):
    return jnp.dot(a, b, preferred_element_type=F32)


def dot_t(a, b):
    return lax.dot_general(a, b, (((1,), (1,)), ((), ())), preferred_element_type=F32)


def silu(x):
    return x / (1.0 + jnp.exp(-x))


def kernel(n_sp, n_tp, names, *refs):
    (
        tokens_hbm,
        gain_hbm,
        wq_hbm,
        wk_hbm,
        wv_hbm,
        wg_hbm,
        w_in_hbm,
        w_forget_hbm,
        b_in_hbm,
        b_forget_hbm,
        extra_hbm,
        init_hbm,
        normal_hbm,
        mem_gain_hbm,
        wpi_hbm,
        wpg_hbm,
        mix_hbm,
        pool_gain_hbm,
        wom_hbm,
        wop_hbm,
        post_hbm,
    ) = refs[:INPUTS]
    out_ref = refs[INPUTS]
    r = types.SimpleNamespace(**dict(zip(names, refs[INPUTS + 1 :])))
    T, D = r.tokens.shape
    H = r.q.shape[0]
    G = r.mix.shape[0]
    heads = r.w_in.shape[0]
    sp = lax.axis_index("sp")
    tp = lax.axis_index("tp")
    head_scale = HEAD_DIM ** (-0.5)
    tiles = T // TILE
    quad = r.e_recv.shape[1]
    rows_own = HEAD_DIM // quad
    quads = n_sp // quad
    my_quad, my_slot = sp // quad, lax.rem(sp, quad)
    part = HEAD_DIM // n_sp

    mem_lanes = pl.ds(pl.multiple_of(tp * H * HEAD_DIM, HEAD_DIM), H * HEAD_DIM)
    pool_lanes = pl.ds(pl.multiple_of(tp * G * GROUP_DIM, GROUP_DIM), G * GROUP_DIM)
    loads = {}

    def load(name, src, dst, slot=None):
        slot = len(loads) if slot is None else slot
        loads[name] = pltpu.make_async_copy(src, dst, r.local_sem.at[slot])
        loads[name].start()

    load("gain", gain_hbm, r.gain)

    def load_tokens(t):
        span = pl.ds(t * TILE, TILE)
        load(("tokens", t), tokens_hbm.at[span], r.tokens.at[span])

    def load_head(name, source, target, h):
        lanes = pl.ds(h * HEAD_DIM, HEAD_DIM)
        load((name, h), source.at[:, lanes], target.at[:, lanes])

    for t in range(tiles // 2):
        load_tokens(t)
    load("w_in", w_in_hbm, r.w_in)
    load("w_forget", w_forget_hbm, r.w_forget)
    load("b_in", b_in_hbm, r.b_in)
    load("b_forget", b_forget_hbm, r.b_forget)
    load_head("wk", wk_hbm, r.wk, 0)
    for t in range(tiles // 2, tiles):
        load_tokens(t)
    load_head("wv", wv_hbm, r.wv, 0)
    load("extra", extra_hbm, r.extra)
    load("normal", normal_hbm, r.normal)
    for h in range(1, H):
        load_head("wk", wk_hbm, r.wk, h)
        load_head("wv", wv_hbm, r.wv, h)
    load("wpi", wpi_hbm, r.wpi)
    load("wq", wq_hbm, r.wq)

    r.ext[0:WIDEST, :] = jnp.zeros((WIDEST, r.ext.shape[1]), BF16)
    barrier = pltpu.get_barrier_semaphore()
    for step in range(1, n_sp):
        pl.semaphore_signal(
            barrier, inc=1, device_id={"sp": lax.rem(sp + step, n_sp)}, device_id_type=MESH
        )
    for step in range(1, n_tp):
        pl.semaphore_signal(
            barrier, inc=1, device_id={"tp": lax.rem(tp + step, n_tp)}, device_id_type=MESH
        )

    def remote(src, dst, send_sem, recv_sem, axis, peer):
        return pltpu.make_async_remote_copy(
            src_ref=src,
            dst_ref=dst,
            send_sem=send_sem,
            recv_sem=recv_sem,
            device_id={axis: peer},
            device_id_type=MESH,
        )

    r.gates_w[...] = jnp.zeros_like(r.gates_w)
    r.gates_b[...] = jnp.zeros_like(r.gates_b)
    r.rows[...] = jnp.zeros_like(r.rows)
    r.a_send[...] = jnp.zeros_like(r.a_send)
    loads["gain"].wait()
    loads["tokens", 0].wait()

    def norm_tile(rows):
        x = r.tokens[rows, :].astype(F32)
        scale = lax.rsqrt(jnp.mean(x * x, axis=-1, keepdims=True) + EPS)
        r.normed[rows, :] = (x * scale * r.gain[...]).astype(BF16)

    def head_lanes(h):
        return slice(h * HEAD_DIM, (h + 1) * HEAD_DIM)

    def whole(ref, h):
        return lambda rows, value: ref.__setitem__((h, rows), value.astype(ref.dtype))

    def gates_product(rows):
        r.cols[rows, :] = dot_t(r.normed[rows, :], r.gates_w[...]) + r.gates_b[...]

    def product(weight, lanes, rows, store):
        store(rows, dot(r.normed[rows, :], weight[:, lanes]))

    per_owner = n_sp // quad
    owner = sp // per_owner
    turn = lax.rem(sp, per_owner)
    init_place = r.init.at[:, pl.ds(pl.multiple_of(turn * part, part), part), :]
    init_copy = remote(
        init_hbm, init_place, r.init_sems.at[per_owner], r.init_sems.at[turn], "sp", owner
    )
    init_local = pltpu.make_async_copy(init_hbm, init_place, r.init_sems.at[per_owner])

    def send_init():
        pl.semaphore_wait(barrier, n_sp - 1 + n_tp - 1)

        @pl.when(owner != sp)
        def _():
            init_copy.start()

        @pl.when(owner == sp)
        def _():
            init_local.start()

    half = tiles // 2
    for t in range(half):
        if t > 0:
            loads["tokens", t].wait()
        for sub in range(0, TILE, SUB):
            norm_tile(pl.ds(t * TILE + sub, SUB))
    for name in ("w_in", "w_forget", "b_in", "b_forget", ("wk", 0)):
        loads[name].wait()
    load("wpg", wpg_hbm, r.wpg, 0)
    load("wg", wg_hbm, r.wg, 1)
    load("mix", mix_hbm.at[pl.ds(tp * G, G)], r.mix, 2)
    load("pool_gain", pool_gain_hbm.at[:, pool_lanes], r.pool_gain, 3)
    load("mem_gain", mem_gain_hbm.at[:, mem_lanes], r.mem_gain, 4)
    load("wop", wop_hbm, r.wop, 5)
    load("wom", wom_hbm, r.wom, 6)
    load("post", post_hbm, r.post, 7)
    r.gates_w[0:heads, :] = r.w_in[...]
    r.gates_w[heads : 2 * heads, :] = r.w_forget[...]
    r.gates_b[:, 0:heads] = r.b_in[...]
    r.gates_b[:, heads : 2 * heads] = r.b_forget[...]
    def early_products(rows):
        gates_product(rows)
        product(r.wk, head_lanes(0), rows, whole(r.k, 0))

    pieces = (slice(0, half * TILE), slice(half * TILE, T))
    loads["tokens", half].wait()
    early_products(pieces[0])
    for t in range(half, tiles):
        if t > half:
            loads["tokens", t].wait()
            if t == half + 1:
                loads["wv", 0].wait()
                for part_rows in (slice(0, TILE), slice(TILE, half * TILE)):
                    product(r.wv, head_lanes(0), part_rows, whole(r.v, 0))
        for sub in range(0, TILE, SUB):
            norm_tile(pl.ds(t * TILE + sub, SUB))
    send_init()
    for name in ("extra", "normal"):
        loads[name].wait()
    for h in range(1, H):
        loads["wk", h].wait()
        loads["wv", h].wait()
    early_products(pieces[1])
    for start in (half * TILE, half * TILE + TILE):
        product(r.wv, head_lanes(0), slice(start, start + TILE), whole(r.v, 0))

    tri = (
        lax.broadcasted_iota(jnp.int32, (TILE, TILE), 0)
        <= lax.broadcasted_iota(jnp.int32, (TILE, TILE), 1)
    ).astype(F32)
    spare = [jnp.zeros((8 - H, TILE), F32)]
    log_keeps = []
    for t in range(tiles):
        span = pl.ds(t * TILE, TILE)
        r.raw[:, span] = r.cols[span, :].T
        own_rows = [r.raw[pl.ds(heads + tp * H + h, 1), span] for h in range(H)]
        added = [r.extra[h : h + 1, span] for h in range(H)]
        raw = jnp.concatenate(own_rows + spare, axis=0)
        log_keep = jnp.minimum(raw, 0.0) - jnp.log1p(jnp.exp(-jnp.abs(raw)))
        log_keeps.append(log_keep + jnp.concatenate(added + spare, axis=0))
    runs = jnp.dot(
        jnp.concatenate(log_keeps, axis=0),
        tri,
        preferred_element_type=F32,
        precision=lax.Precision.HIGHEST,
    )
    last = [runs[8 * t : 8 * t + 8, TILE - 1 : TILE] for t in range(tiles)]
    carry = jnp.zeros((8, 1), F32)
    for t in range(tiles):
        span = pl.ds(t * TILE, TILE)
        run = carry + runs[8 * t : 8 * t + 8]
        carry = carry + last[t]
        for h in range(H):
            keep = run[h : h + 1]
            r.rows[h : h + 1, span] = r.raw[pl.ds(tp * H + h, 1), span] - keep
            r.rows[H + h : H + h + 1, span] = keep
    for t in range(tiles):
        span = pl.ds(t * TILE, TILE)
        r.cols[span, :] = r.rows[:, span].T

    def a_copy(h, step):
        peer = lax.rem(sp + step, n_sp)
        return remote(
            r.a_send.at[h], r.a_recv.at[sp, h], r.a_sems.at[0, h], r.a_sems.at[1, h], "sp", peer
        )

    def s_copy(h, step):
        peer = lax.rem(my_slot + step, quad)
        return remote(
            r.s_send.at[h, peer],
            r.s_recv.at[h, my_slot],
            r.s_sems.at[0, h],
            r.s_sems.at[1, h],
            "sp",
            my_quad * quad + peer,
        )

    def e_copy(h, step):
        peer = lax.rem(my_slot + step, quad)
        return remote(
            r.e_send.at[h, peer],
            r.e_recv.at[h, my_slot],
            r.e_sems.at[0, h],
            r.e_sems.at[1, h],
            "sp",
            my_quad * quad + peer,
        )

    def all_of(ref, sems, axis="sp"):
        peer = lax.rem(sp + 1, n_sp) if axis == "sp" else lax.rem(tp + 1, n_tp)
        return remote(ref, ref, sems[0], sems[1], axis, peer)

    def t_copy(h):
        return remote(
            r.t_send.at[h],
            r.t_recv.at[h],
            r.t_sems.at[0, h],
            r.t_sems.at[1, h],
            "sp",
            lax.rem(sp + quad, n_sp),
        )

    for h in range(H):
        if h > 0:
            for rows in pieces:
                product(r.wk, head_lanes(h), rows, whole(r.k, h))
            for rows in pieces:
                product(r.wv, head_lanes(h), rows, whole(r.v, h))
        a_max = jnp.max(r.rows[h : h + 1, :], axis=-1, keepdims=True)
        total = r.rows[H + h : H + h + 1, T - 1 : T]
        state = jnp.zeros((HEAD_DIM, HEAD_DIM), F32)
        normal = jnp.zeros((1, HEAD_DIM), F32)
        for t in range(tiles):
            span = pl.ds(t * TILE, TILE)
            weight = jnp.exp(r.cols[span, h : h + 1] - a_max)
            kw = weight * r.k[h, span, :].astype(F32)
            normal = normal + jnp.sum(kw, axis=0, keepdims=True)
            state = state + lax.dot_general(
                kw.astype(BF16),
                r.v[h, span, :],
                (((0,), (0,)), ((), ())),
                preferred_element_type=F32,
            )
        r.s_send[h] = state.reshape(quad, rows_own, HEAD_DIM).astype(BF16)
        r.a_send[h, 0:1, :] = jnp.broadcast_to(total + a_max, (1, HEAD_DIM))
        r.a_send[h, 1:2, :] = jnp.broadcast_to(total, (1, HEAD_DIM))
        r.a_send[h, 2:3, :] = normal
        r.a_send[h, 3:4, 0:part] = r.normal[h : h + 1, :]
        for step in range(1, n_sp):
            a_copy(h, step).start()
        for step in range(1, quad):
            s_copy(h, step).start()
        r.s_recv[h, my_slot] = r.s_send[h, my_slot]
        r.a_recv[sp, h] = r.a_send[h]

    def m_row(h, j):
        return pl.ds(h * (n_sp + 1) + j, 1)

    def chain(h):
        all_of(r.a_recv.at[pl.ds(0, n_sp - 1), h], (r.a_sems.at[0, h], r.a_sems.at[1, h])).wait()
        for j in range(n_sp):
            r.start[h : h + 1, j * part : (j + 1) * part] = r.a_recv[j, h, 3:4, 0:part]
        normal = r.start[h : h + 1, :]
        stab = jnp.zeros((1, HEAD_DIM), F32)
        my_stab, my_normal = stab, normal
        for j in range(n_sp):
            r.m[m_row(h, j), :] = stab
            if j > 0:
                my_stab = jnp.where(sp == j, stab, my_stab)
                my_normal = jnp.where(sp == j, normal, my_normal)
            late = r.a_recv[j, h, 0:1, :]
            keep = r.a_recv[j, h, 1:2, :]
            joint = jnp.maximum(late, keep + stab)
            normal = normal * jnp.exp(keep + stab - joint) + r.a_recv[j, h, 2:3, :] * jnp.exp(
                late - joint
            )
            stab = joint
        r.m[m_row(h, n_sp), :] = stab
        r.enter[h : h + 1, :] = my_stab
        r.enter[H + h : H + h + 1, :] = my_normal

    def spread(h):
        state = r.state[h]
        for i in range(quad):
            j = my_quad * quad + i
            r.e_send[h, i] = state.astype(BF16)
            stab, joint = r.m[m_row(h, j), :], r.m[m_row(h, j + 1), :]
            late = r.a_recv[j, h, 0:1, :]
            keep = r.a_recv[j, h, 1:2, :]
            state = state * jnp.exp(keep + stab - joint) + r.s_recv[h, i].astype(F32) * jnp.exp(
                late - joint
            )
        r.t_send[h] = state.astype(BF16)

        @pl.when(my_quad < quads - 1)
        def _():
            t_copy(h).start()

        for step in range(1, quad):
            e_copy(h, step).start()
        r.e_recv[h, my_slot] = r.e_send[h, my_slot]

    def gathered(h):
        chain(h)
        all_of(r.s_recv.at[h, pl.ds(0, quad - 1)], (r.s_sems.at[0, h], r.s_sems.at[1, h])).wait()

        @pl.when(my_quad == 0)
        def _():
            if h == 0:
                for turn_in in range(per_owner):
                    source = sp * per_owner + turn_in

                    @pl.when(source != sp)
                    def _():
                        init_copy_from(turn_in).wait_recv()

                @pl.when(owner == sp)
                def _():
                    init_local.wait()

            r.state[h] = r.init[h]
            spread(h)

    def init_copy_from(turn_in):
        place = r.init.at[:, pl.ds(turn_in * part, part), :]
        return remote(init_hbm, place, r.init_sems.at[per_owner], r.init_sems.at[turn_in], "sp", owner)

    def carried_on(h):
        @pl.when(my_quad > 0)
        def _():
            t_copy(h).wait_recv()
            r.state[h] = r.t_recv[h].astype(F32)
            spread(h)

    loads["wpi"].wait()
    loads["wq"].wait()

    def store_pool(rows, value):
        r.ext[WIDEST + rows.start : WIDEST + rows.stop, :] = value.astype(BF16)

    for rows in pieces:
        product(r.wpi, slice(None), rows, store_pool)

    def halo_copy(member):
        width = min(WIDEST, max(16, 2 ** (G * (member + 1))))
        return remote(
            r.ext.at[pl.ds(T + WIDEST - width, width)],
            r.ext.at[pl.ds(WIDEST - width, width)],
            r.halo_sems.at[0],
            r.halo_sems.at[1],
            "sp",
            lax.rem(sp + 1, n_sp),
        )

    for member in range(n_tp):

        @pl.when((tp == member) & (sp < n_sp - 1))
        def _(member=member):
            halo_copy(member).start()


    def query_to(h):
        def store(rows, value):
            r.q[h, rows, :] = value.astype(BF16) * head_scale

        return store

    for rows in pieces:
        product(r.wq, head_lanes(0), rows, query_to(0))
    gathered(0)
    for h in range(1, H):
        for rows in pieces:
            product(r.wq, head_lanes(h), rows, query_to(h))
    for name in ("wg", "mem_gain", "wpg", "pool_gain", "mix", "wop", "wom", "post"):
        loads[name].wait()
    chips = n_tp // 2
    chip, core = tp // 2, lax.rem(tp, 2)
    sibling = chip * 2 + 1 - core
    block = T // n_tp
    segment = 2 * block
    unit = block // sum(SHARES)
    chunks = []
    for share in SHARES:
        begin = chunks[-1][0] + chunks[-1][1] if chunks else 0
        chunks.append((begin, share * unit))
    count = len(chunks)
    extra_slot = chips * count
    lead = chunks[0][1]

    def chunk_rows(target, which, n):
        begin, size = chunks[n]
        return pl.ds(pl.multiple_of((target * 2 + which) * block + begin, unit), size)

    first_target = lax.rem(chip + 1, chips)
    lead_theirs = chunk_rows(first_target, 1 - core, 0)
    lead_ours = chunk_rows(first_target, core, 0)

    def gate_to(h):
        def store(rows, value):
            r.gate[h, rows, :] = r.mem_gain[:, head_lanes(h)] * silu(value)

        return store

    def store_gate(rows, value):
        r.pgate[rows, :] = r.pool_gain[...] * silu(value)

    def gates_of(target):
        start = pl.multiple_of(target * segment, segment)
        for h in range(H):
            product(r.wg, head_lanes(h), pl.ds(start, segment), gate_to(h))
        for piece in range(2):
            rows = pl.ds(pl.multiple_of(start + piece * block, block), block)
            product(r.wpg, slice(None), rows, store_gate)

    def lead_pair(ref):
        return jnp.concatenate([ref[lead_theirs, :], ref[lead_ours, :]], axis=0)

    def pool_rows(start, size):
        for g in range(G):
            window = jnp.left_shift(2, tp * G + g)
            offset = (
                lax.broadcasted_iota(jnp.int32, (size, size + WIDEST), 0)
                + WIDEST
                - lax.broadcasted_iota(jnp.int32, (size, size + WIDEST), 1)
            )
            band = jnp.where((offset >= 0) & (offset < window), 1.0, 0.0).astype(BF16)
            lanes = slice(g * GROUP_DIM, (g + 1) * GROUP_DIM)
            span = pl.ds(start, size)
            here = r.ext[pl.ds(pl.multiple_of(start + WIDEST, unit), size), lanes]
            before = r.ext[pl.ds(start, WIDEST), lanes]
            sums = dot(band[:, :WIDEST], before) + dot(band[:, WIDEST:], here)
            position = lax.broadcasted_iota(jnp.int32, (size, 1), 0) + (sp * T + start + 1)
            counts = jnp.minimum(position, window).astype(F32)
            pooled = (sums / counts - here.astype(F32)).astype(BF16)
            r.pool[span, lanes] = (dot(pooled, r.mix[g]) * r.pgate[span, lanes]).astype(BF16)

    def pool_of(target):
        for piece in range(segment // TILE):
            pool_rows(pl.multiple_of(target * segment + piece * TILE, TILE), TILE)

    value = dot(lead_pair(r.normed), r.wpg[...])
    store_gate(lead_theirs, value[:lead])
    store_gate(lead_ours, value[lead:])
    value = dot(lead_pair(r.normed), r.wg[...])
    for h in range(H):
        gate_to(h)(lead_theirs, value[:lead, head_lanes(h)])
        gate_to(h)(lead_ours, value[lead:, head_lanes(h)])
    for h in range(1, H):
        gathered(h)
    for member in range(n_tp):

        @pl.when((tp == member) & (sp > 0))
        def _(member=member):
            halo_copy(member).wait_recv()

    def lead_pool(which):
        pool_rows(pl.multiple_of((first_target * 2 + which) * block, block), lead)

    lead_pool(1 - core)
    def memory_product(rows, entering=None):
        values = [r.num[h, rows, :] for h in range(H)]
        if entering is not None:
            carried = dot(r.q[H - 1, rows, :], entering)
            values[-1] = values[-1] + r.beta[H - 1, rows, :] * carried
        parts = [(values[h] * r.gate[h, rows, :]).astype(BF16) for h in range(H)]
        return dot(parts[0] if H == 1 else jnp.concatenate(parts, axis=1), r.wom[...])

    def finish(rows):
        pool = dot(r.pool[rows, :], r.wop[...])
        return (memory_product(rows) * r.scale[rows, 0:1] + pool).astype(BF16)

    jobs = []
    for j in range(1, chips + 1):
        for n in range(count):
            jobs.append((j, n, lax.rem(chip + j, chips)))

    siblings, links = {}, {}

    def place(j, n):
        if n < 0:
            return pl.ds(chips * block, lead)
        begin, size = chunks[n]
        return pl.ds((j - 1) * block + begin, size)

    def to_sibling(j, n):
        slot = extra_slot if n < 0 else (j - 1) * count + n
        rows = place(j, n)
        siblings[j, n] = remote(
            r.sib_send.at[rows],
            r.sib_recv.at[rows],
            r.sib_sems.at[extra_slot + 1],
            r.sib_sems.at[slot],
            "tp",
            sibling,
        )
        siblings[j, n].start()

    def to_chip(j, n, target):
        slot = extra_slot - count if n < 0 else (j - 1) * count + n
        rows = place(j, n)
        links[j, n] = remote(
            r.link_send.at[rows],
            r.link_recv.at[rows],
            r.link_sems.at[extra_slot - count + 1],
            r.link_sems.at[slot],
            "tp",
            target * 2 + core,
        )
        links[j, n].start()

    r.sib_send[place(1, -1), :] = dot(r.pool[lead_theirs, :], r.wop[...]).astype(BF16)
    to_sibling(1, -1)
    lead_pool(core)
    r.lead[...] = dot(r.pool[lead_ours, :], r.wop[...])

    def pass_on(j, n, target):
        siblings[j, n].wait_recv()
        rows = place(j, n)
        mine = r.lead[...] if (j, max(n, 0)) == (1, 0) else r.own[rows, :].astype(F32)
        r.link_send[rows, :] = (mine + r.sib_recv[rows, :].astype(F32)).astype(BF16)
        to_chip(j, n, target)

    carried_on(0)
    diag_mask = lax.broadcasted_iota(jnp.int32, (TILE, TILE), 0) >= lax.broadcasted_iota(
        jnp.int32, (TILE, TILE), 1
    )

    def attend(h, members):
        enter_max = r.enter[h : h + 1, 0:1]
        enter_normal = r.enter[H + h : H + h + 1, :]
        for t in members:
            span = pl.ds(t * TILE, TILE)
            queries = r.q[h, span, :]
            near = jnp.where(diag_mask, r.rows[h : h + 1, span], FLOOR)
            top = jnp.max(near, axis=-1, keepdims=True)
            if t > 0:
                far = r.rows[h : h + 1, 0 : t * TILE]
                top = jnp.maximum(top, jnp.max(far, axis=-1, keepdims=True))
            weights = jnp.exp(near - top) * dot_t(queries, r.k[h, span, :])
            den = jnp.sum(weights, axis=-1, keepdims=True)
            num = dot(weights.astype(BF16), r.v[h, span, :])
            if t > 0:
                weights = jnp.exp(far - top) * dot_t(queries, r.k[h, 0 : t * TILE, :])
                den = den + jnp.sum(weights, axis=-1, keepdims=True)
                num = num + dot(weights.astype(BF16), r.v[h, 0 : t * TILE, :])
            keep = r.cols[span, H + h : H + h + 1]
            row_max = keep + top
            carried = keep + enter_max
            joint = jnp.maximum(row_max, carried)
            local_weight = jnp.exp(row_max - joint)
            carry_weight = jnp.exp(carried - joint)
            den = den * local_weight + carry_weight * jnp.sum(
                queries.astype(F32) * enter_normal, axis=-1, keepdims=True
            )
            bound = jnp.maximum(jnp.abs(den), jnp.exp(-joint))
            r.num[h, span, :] = num * (local_weight / bound)
            r.beta[h, span, :] = carry_weight / bound

    attend(0, range(tiles // 2))
    pass_on(1, -1, first_target)
    attend(0, range(tiles // 2, tiles))
    for h in range(1, H):
        carried_on(h)

    for h in range(1, H):
        attend(h, range(tiles))
    def combine(h):
        state = r.e_recv[h].reshape(HEAD_DIM, HEAD_DIM)
        for t in range(tiles):
            span = slice(t * TILE, (t + 1) * TILE)
            carried = dot(r.q[h, span, :], state)
            memory = r.num[h, span, :] + r.beta[h, span, :] * carried
            r.num[h, span, :] = memory
            squares = jnp.sum(memory * memory, axis=-1, keepdims=True)
            if h > 0:
                squares = squares + r.squares[span]
            if h < H - 1:
                r.squares[span] = squares
            else:
                r.sq_send[:, span] = jnp.broadcast_to(squares, (TILE, 128)).T[0:1]

    for h in range(H):
        all_of(r.e_recv.at[h, pl.ds(0, quad - 1)], (r.e_sems.at[0, h], r.e_sems.at[1, h])).wait()
        if h < H - 1:
            combine(h)
    entering = r.e_recv[H - 1].reshape(HEAD_DIM, HEAD_DIM)
    r.sib_send[place(1, 0), :] = memory_product(lead_theirs, entering).astype(BF16)
    to_sibling(1, 0)
    combine(H - 1)
    for step in range(1, n_tp):
        remote(
            r.sq_send,
            r.sq_recv.at[step],
            r.sq_sems.at[0],
            r.sq_sems.at[1],
            "tp",
            lax.rem(tp + step, n_tp),
        ).start()
    r.lead[...] = memory_product(lead_ours)
    pass_on(1, 0, first_target)
    for j in range(1, chips):
        gates_of(lax.rem(chip + j, chips))
        pool_of(lax.rem(chip + j, chips))
    all_of(r.sq_recv.at[pl.ds(0, n_tp - 1)], (r.sq_sems.at[0], r.sq_sems.at[1]), "tp").wait()
    for t in range(tiles):
        span = pl.ds(t * TILE, TILE)
        total = r.sq_send[0:1, span]
        for step in range(1, n_tp):
            total = total + r.sq_recv[step, 0:1, span]
        scale = lax.rsqrt(total / (HEAD_DIM * H * n_tp) + EPS)
        r.scale[span, :] = jnp.broadcast_to(scale, (128, TILE)).T

    for index, (j, n, target) in enumerate(jobs):
        if index == 0:
            continue
        if j == chips and n == 0:
            gates_of(chip)
            pool_of(chip)
        r.sib_send[place(j, n), :] = finish(chunk_rows(target, 1 - core, n))
        to_sibling(j, n)
        r.own[place(j, n), :] = finish(chunk_rows(target, core, n))
        if index == 1 and j < chips:
            pass_on(j, n, target)
        elif index > 2 and jobs[index - 1][0] < chips:
            pass_on(*jobs[index - 1])
    own_scale = r.scale.at[pl.ds(pl.multiple_of(tp * block, block), lead)]
    for n in range(count):
        siblings[chips, n].wait_recv()
        begin, size = chunks[n]
        total = r.own[place(chips, n), :].astype(F32) + r.sib_recv[place(chips, n), :].astype(F32)
        for j in range(1, chips):
            links[j, n].wait_recv()
            came = r.link_recv[place(j, n), :].astype(F32)
            if (j, n) == (1, 0):
                links[1, -1].wait_recv()
                came = came * own_scale[:, 0:1] + r.link_recv[place(1, -1), :].astype(F32)
            total = total + came
        scale = lax.rsqrt(jnp.mean(total * total, axis=-1, keepdims=True) + EPS)
        out_ref[begin : begin + size, :] = (total * scale * r.post[...]).astype(BF16)
    for member in range(n_tp):

        @pl.when((tp == member) & (sp < n_sp - 1))
        def _(member=member):
            halo_copy(member).wait_send()


    @pl.when(owner != sp)
    def _():
        init_copy.wait_send()

    for h in range(H):
        @pl.when(my_quad < quads - 1)
        def _(h=h):
            t_copy(h).wait_send()

    sent = r.sib_send.at[pl.ds(0, chips * block + lead)]
    all_of(sent, (r.sib_sems.at[extra_slot + 1], r.sib_sems.at[0]), "tp").wait_send()
    sent = r.link_send.at[pl.ds(0, (chips - 1) * block + lead)]
    all_of(sent, (r.link_sems.at[extra_slot - count + 1], r.link_sems.at[0]), "tp").wait_send()


def body(
    n_sp,
    n_tp,
    tokens,
    pre_gain,
    w_query,
    w_key,
    w_value,
    memory_output_gate_weight,
    w_input_gate,
    w_forget_gate,
    input_bias,
    forget_bias,
    forget_extra,
    initial_memory,
    initial_normal,
    memory_gain,
    w_pool_input,
    w_pool_gate,
    pool_mix,
    pool_gain,
    w_out_memory,
    w_out_pool,
    post_gain,
):
    T, D = tokens.shape
    MW = w_query.shape[1]
    PW = w_pool_input.shape[1]
    H = MW // HEAD_DIM
    G = PW // GROUP_DIM
    heads = w_input_gate.shape[1]
    part = initial_normal.shape[1]
    quad = min(QUAD, n_sp)
    rows_own = HEAD_DIM // quad
    chips = n_tp // 2
    block = T // n_tp
    slots = chips * len(SHARES)
    lead = block // sum(SHARES) * SHARES[0]
    hbm = pl.BlockSpec(memory_space=pl.ANY)
    V = pltpu.VMEM
    dma = pltpu.SemaphoreType.DMA
    scratch = dict(
        tokens=V((T, D), BF16),
        gain=V((1, D), F32),
        wq=V((D, MW), BF16),
        wk=V((D, MW), BF16),
        wv=V((D, MW), BF16),
        wg=V((D, MW), BF16),
        w_in=V((heads, D), BF16),
        w_forget=V((heads, D), BF16),
        b_in=V((1, heads), F32),
        b_forget=V((1, heads), F32),
        extra=V((H, T), F32),
        normal=V((H, part), F32),
        mem_gain=V((1, MW), F32),
        wpi=V((D, PW), BF16),
        wpg=V((D, PW), BF16),
        mix=V((G, GROUP_DIM, GROUP_DIM), BF16),
        pool_gain=V((1, PW), F32),
        wom=V((MW, D), BF16),
        wop=V((PW, D), BF16),
        post=V((1, D), F32),
        normed=V((T, D), BF16),
        q=V((H, T, HEAD_DIM), BF16),
        k=V((H, T, HEAD_DIM), BF16),
        v=V((H, T, HEAD_DIM), BF16),
        gate=V((H, T, HEAD_DIM), F32),
        pgate=V((T, PW), F32),
        ext=V((T + WIDEST, PW), BF16),
        pool=V((T, PW), BF16),
        rows=V((128, T), F32),
        cols=V((T, 128), F32),
        num=V((H, T, HEAD_DIM), F32),
        beta=V((H, T, 1), F32),
        gates_w=V((128, D), BF16),
        gates_b=V((1, 128), F32),
        raw=V((128, T), F32),
        start=V((8, HEAD_DIM), F32),
        enter=V((2 * H, HEAD_DIM), F32),
        m=V((H * (n_sp + 1), HEAD_DIM), F32),
        init=V((H, rows_own, HEAD_DIM), F32),
        state=V((H, rows_own, HEAD_DIM), F32),
        a_send=V((H, 4, HEAD_DIM), F32),
        a_recv=V((n_sp, H, 4, HEAD_DIM), F32),
        s_send=V((H, quad, rows_own, HEAD_DIM), BF16),
        s_recv=V((H, quad, rows_own, HEAD_DIM), BF16),
        e_send=V((H, quad, rows_own, HEAD_DIM), BF16),
        e_recv=V((H, quad, rows_own, HEAD_DIM), BF16),
        t_send=V((H, rows_own, HEAD_DIM), BF16),
        t_recv=V((H, rows_own, HEAD_DIM), BF16),
        squares=V((T, 1), F32),
        sq_send=V((1, T), F32),
        sq_recv=V((n_tp, 1, T), F32),
        lead=V((lead, D), F32),
        scale=V((T, 128), F32),
        sib_send=V((chips * block + lead, D), BF16),
        sib_recv=V((chips * block + lead, D), BF16),
        own=V((chips * block, D), BF16),
        link_send=V((chips * block + lead, D), BF16),
        link_recv=V((chips * block + lead, D), BF16),
        local_sem=dma((INPUTS - 8 + T // TILE + 2 * H,)),
        init_sems=dma((n_sp // quad + 1,)),
        a_sems=dma((2, H)),
        s_sems=dma((2, H)),
        e_sems=dma((2, H)),
        t_sems=dma((2, H)),
        halo_sems=dma((2,)),
        sq_sems=dma((2,)),
        sib_sems=dma((slots + 2,)),
        link_sems=dma((slots - len(SHARES) + 2,)),
    )
    return pl.pallas_call(
        functools.partial(kernel, n_sp, n_tp, tuple(scratch)),
        out_shape=pltpu.VMEM((block, D), BF16),
        in_specs=[hbm] * INPUTS,
        out_specs=pl.BlockSpec(memory_space=pltpu.VMEM),
        scratch_shapes=list(scratch.values()),
        compiler_params=pltpu.CompilerParams(
            collective_id=0, has_side_effects=True, vmem_limit_bytes=60 * 1024 * 1024
        ),
    )(
        tokens,
        pre_gain[None],
        w_query,
        w_key,
        w_value,
        memory_output_gate_weight,
        w_input_gate.T,
        w_forget_gate.T,
        input_bias[None],
        forget_bias[None],
        forget_extra.T,
        initial_memory,
        initial_normal,
        memory_gain[None],
        w_pool_input,
        w_pool_gate,
        pool_mix,
        pool_gain[None],
        w_out_memory,
        w_out_pool,
        post_gain[None],
    )


def solution(mesh):
    in_specs = (
        P("sp", None),
        P(),
        P(None, "tp"),
        P(None, "tp"),
        P(None, "tp"),
        P(None, "tp"),
        P(),
        P(),
        P(),
        P(),
        P("sp", "tp"),
        P("tp", "sp", None),
        P("tp", "sp"),
        P(),
        P(None, "tp"),
        P(None, "tp"),
        P(),
        P(),
        P("tp", None),
        P("tp", None),
        P(),
    )
    out_specs = P(("sp", "tp"), None)
    sizes = dict(mesh.shape)
    run = functools.partial(body, sizes["sp"], sizes["tp"])
    return jax.shard_map(run, mesh=mesh, in_specs=in_specs, out_specs=out_specs, check_vma=False)
```
